32 devices in a mesh: rep: 2 (over core), fs: 8 (over z, y), tp: 2 (over x).
Axes of the slice: x: 2, y: 2, z: 4, core: 2. Of those that a mesh axis runs over, the one named last changes fastest.
Arguments:
- residual: bfloat16 [2048, 4096], P('tp', ('rep', 'fs')), may hold values from -6 to 6
- mixer_gain: float32 [2048], replicated, may hold values from 0.1 to 1.9
- value_weight: float32 [2048, 512], P('fs', 'tp'), may hold values from -0.125 to 0.125
- value_scale: float32 [512], P('tp'), may hold values from 0.2 to 8, as said below
- input_gate_weight: float32 [2048, 512], P('fs', 'tp'), may hold values from -0.125 to 0.125
- input_gate_scale: float32 [512], P('tp'), may hold values from 0.5 to 2
- output_gate_weight: float32 [2048, 512], P('fs', 'tp'), may hold values from -0.125 to 0.125
- output_gate_scale: float32 [512], P('tp'), may hold values from 0.5 to 2
- conv_taps: float32 [3, 512], P(None, 'tp'), may hold values from -3 to 3
- conv_gain: float32 [512], P('tp'), may hold values from 0.1 to 1.9
- mixer_out_weight: float32 [512, 2048], P('tp', 'fs'), may hold values from -0.25 to 0.25
- mixer_out_scale: float32 [2048], P('fs'), may hold values from 0.5 to 2
- channel_gain: float32 [2048], replicated, may hold values from 0.1 to 1.9
- gate_weight: float32 [2048, 5632], P('fs', 'tp'), may hold values from -0.125 to 0.125
- gate_scale: float32 [5632], P('tp'), may hold values from 0.5 to 2
- up_weight: float32 [2048, 5632], P('fs', 'tp'), may hold values from -0.125 to 0.125
- up_scale: float32 [5632], P('tp'), may hold values from 0.5 to 2
- down_weight: float32 [5632, 2048], P('tp', 'fs'), may hold values from -0.078125 to 0.078125
- down_scale: float32 [2048], P('fs'), may hold values from 0.5 to 2
Outputs:
- layer_out: bfloat16 [2048, 4096], P('tp', ('rep', 'fs'))
The draws below stay inside these ranges and needn't reach their ends.
Inputs may be any that keep to these rules, and one draw needn't show every extreme that they name: `value_scale`: positive column scales.
All inputs are finite; a program needn't handle non-finite values.
Results may differ from the reference program's by a relative error of at most 0.018.
Values may be sent and summed in bfloat16 or wider, within the bound.
No kernel may reach another device: no remote copies, remote signals or barrier semaphores. Data moves between devices by JAX's collectives and lax.ppermute only.
A program may use at most 128 MiB of HBM per device.

```python
import math
import jax
import jax.numpy as jnp
from jax import lax

D = 2048
C = 512
FF = 5632
TAPS = 3
LEN = 128
TOKENS = 4096
N_TP = 2


def draw_value_scale(key, part):
    index = jnp.arange(C, dtype=jnp.float32)
    ramp = 4.0 ** (index / C)
    rough = jnp.exp(jax.random.uniform(key, (C,), jnp.float32, -0.7, 0.7))
    return (0.5 * ramp * rough).astype(jnp.float32)


def shard_levels(own_key, shape, split, smallest, top_value):
    loudness = 1.0
    for dim, shards_of in split:
        heights = jax.random.uniform(jax.random.fold_in(jax.random.fold_in(own_key, 6), dim), (shards_of,), jnp.float32, smallest / len(split), top_value / len(split))
        loudness = loudness * jnp.repeat(jnp.exp(heights), shape[dim] // shards_of).reshape((-1,) + (1,) * (len(shape) - 1 - dim))
    return loudness


def scatter_about(own_key, extent, scale, most, pieces=(), kind=jnp.bfloat16):
    factor_of = shard_levels(own_key, extent, pieces, -0.22, 0.18) if pieces else 1.0
    values = jax.random.normal(own_key, extent, jnp.float32) * scale * factor_of
    return jnp.minimum(jnp.maximum(values, -most), most).astype(kind)


def setup_inputs(seed: int = 0) -> dict:
    key_of = jax.random.split(jax.random.key(seed), 20)
    residual = scatter_about(key_of[0], (D, TOKENS), 1.0, 6.0, ((0, 2), (1, 16)))
    mixer_gain = jnp.clip(1.0 + 0.18 * jax.random.normal(key_of[1], (D,), jnp.float32), 0.1, 1.9)
    value_weight = scatter_about(key_of[2], (D, C), D ** -0.5, 0.125, ((0, 8), (1, 2)), jnp.float32)
    value_scale = draw_value_scale(jax.random.fold_in(key_of[19], 71), 0)
    input_gate_weight = scatter_about(key_of[4], (D, C), D ** -0.5, 0.125, ((0, 8), (1, 2)), jnp.float32)
    input_gate_scale = jnp.clip(jnp.exp(math.log(2.0) - 1.3862944 * jax.random.uniform(key_of[5], (C,), jnp.float32) ** shard_levels(key_of[5], (C,), ((0, 2),), -0.2, 0.2)), 0.5, 2.0)
    output_gate_weight = scatter_about(key_of[6], (D, C), D ** -0.5, 0.125, ((0, 8), (1, 2)), jnp.float32)
    output_gate_scale = jnp.clip(jnp.exp(math.log(2.0) - 1.3862944 * jax.random.uniform(key_of[7], (C,), jnp.float32) ** shard_levels(key_of[7], (C,), ((0, 2),), -0.2, 0.2)), 0.5, 2.0)
    conv_taps = scatter_about(key_of[8], (TAPS, C), 0.577, 3.0, ((1, 2),), jnp.float32)
    conv_gain = jnp.clip(1.0 + 0.18 * jax.random.normal(key_of[9], (C,), jnp.float32), 0.1, 1.9)
    mixer_out_weight = scatter_about(key_of[10], (C, D), C ** -0.5, 0.25, ((0, 2), (1, 8)), jnp.float32)
    mixer_out_scale = jnp.clip(jnp.exp(math.log(2.0) - 1.3862944 * jax.random.uniform(key_of[11], (D,), jnp.float32) ** shard_levels(key_of[11], (D,), ((0, 8),), -0.2, 0.2)), 0.5, 2.0)
    channel_gain = jnp.clip(1.0 + 0.18 * jax.random.normal(key_of[12], (D,), jnp.float32), 0.1, 1.9)
    gate_weight = scatter_about(key_of[13], (D, FF), D ** -0.5, 0.125, ((0, 8), (1, 2)), jnp.float32)
    gate_scale = jnp.clip(jnp.exp(math.log(2.0) - 1.3862944 * jax.random.uniform(key_of[14], (FF,), jnp.float32) ** shard_levels(key_of[14], (FF,), ((0, 2),), -0.2, 0.2)), 0.5, 2.0)
    up_weight = scatter_about(key_of[15], (D, FF), D ** -0.5, 0.125, ((0, 8), (1, 2)), jnp.float32)
    up_scale = jnp.clip(jnp.exp(math.log(2.0) - 1.3862944 * jax.random.uniform(key_of[16], (FF,), jnp.float32) ** shard_levels(key_of[16], (FF,), ((0, 2),), -0.2, 0.2)), 0.5, 2.0)
    down_weight = scatter_about(key_of[17], (FF, D), FF ** -0.5, 0.078125, ((0, 2), (1, 8)), jnp.float32)
    down_scale = jnp.clip(jnp.exp(math.log(2.0) - 1.3862944 * jax.random.uniform(key_of[18], (D,), jnp.float32) ** shard_levels(key_of[18], (D,), ((0, 8),), -0.2, 0.2)), 0.5, 2.0)
    return dict(residual=residual, mixer_gain=mixer_gain, value_weight=value_weight, value_scale=value_scale, input_gate_weight=input_gate_weight, input_gate_scale=input_gate_scale, output_gate_weight=output_gate_weight, output_gate_scale=output_gate_scale, conv_taps=conv_taps, conv_gain=conv_gain, mixer_out_weight=mixer_out_weight, mixer_out_scale=mixer_out_scale, channel_gain=channel_gain, gate_weight=gate_weight, gate_scale=gate_scale, up_weight=up_weight, up_scale=up_scale, down_weight=down_weight, down_scale=down_scale)


epsilon = 1e-06

def normalize(values, gain):
    floats = values.astype(jnp.float32)
    mean = lax.optimization_barrier(jnp.mean(floats * floats, axis=0, keepdims=True))
    return (floats * lax.rsqrt(mean + epsilon) * gain[:, None]).astype(jnp.bfloat16)

def project(weight, rows):
    return jnp.dot(weight.T, rows, preferred_element_type=jnp.float32)

def causal_conv(values, taps):
    total = values.shape[1]
    position = jnp.arange(total, dtype=jnp.int32) % LEN
    shifted_one = jnp.pad(values, ((0, 0), (1, 0)))[:, :total]
    shifted_two = jnp.pad(values, ((0, 0), (2, 0)))[:, :total]
    shifted_one = jnp.where(position[None, :] >= 1, shifted_one, 0.0)
    shifted_two = jnp.where(position[None, :] >= 2, shifted_two, 0.0)
    return taps[2][:, None] * values + taps[1][:, None] * shifted_one + taps[0][:, None] * shifted_two

def block_sum(weight, rows, scale):
    width = weight.shape[0] // N_TP
    total = jnp.zeros((weight.shape[1], rows.shape[1]), jnp.float32)
    for block_index in range(N_TP):
        lower = block_index * width
        part = project(weight[lower:lower + width], rows[lower:lower + width]) * scale[:, None]
        rounded = lax.optimization_barrier(part.astype(jnp.bfloat16))
        total = total + rounded.astype(jnp.float32)
    return total

def reference(residual, mixer_gain, value_weight, value_scale, input_gate_weight, input_gate_scale, output_gate_weight, output_gate_scale, conv_taps, conv_gain, mixer_out_weight, mixer_out_scale, channel_gain, gate_weight, gate_scale, up_weight, up_scale, down_weight, down_scale):
    normed = normalize(residual, mixer_gain)
    value = project(value_weight.astype(jnp.bfloat16), normed) * value_scale[:, None]
    in_gate = project(input_gate_weight.astype(jnp.bfloat16), normed) * input_gate_scale[:, None]
    out_gate = project(output_gate_weight.astype(jnp.bfloat16), normed) * output_gate_scale[:, None]
    mixed = out_gate * causal_conv(in_gate * value, conv_taps)
    mean = lax.optimization_barrier(jnp.mean(mixed * mixed, axis=0, keepdims=True))
    conv_normed = (mixed * lax.rsqrt(mean + epsilon) * conv_gain[:, None]).astype(jnp.bfloat16)
    total = block_sum(mixer_out_weight.astype(jnp.bfloat16), conv_normed, mixer_out_scale)
    after_mixer = (residual.astype(jnp.float32) + total).astype(jnp.bfloat16)
    normed_two = normalize(after_mixer, channel_gain)
    gate = project(gate_weight.astype(jnp.bfloat16), normed_two) * gate_scale[:, None]
    upper = project(up_weight.astype(jnp.bfloat16), normed_two) * up_scale[:, None]
    hidden = (jax.nn.silu(gate) * upper).astype(jnp.bfloat16)
    total_two = block_sum(down_weight.astype(jnp.bfloat16), hidden, down_scale)
    return (after_mixer.astype(jnp.float32) + total_two).astype(jnp.bfloat16)
```

```python
import functools

import jax
import jax.numpy as jnp
from jax import lax
from jax.experimental import pallas as pl
from jax.experimental.pallas import tpu as pltpu
from jax.sharding import Mesh
from jax.sharding import PartitionSpec as P

LEN = 128


epsilon = 1e-06


def normalize(values, gain):
    floats = values.astype(jnp.float32)
    mean = jnp.mean(floats * floats, axis=0, keepdims=True)
    return (floats * lax.rsqrt(mean + epsilon) * gain[:, None]).astype(jnp.bfloat16)


def contract(weight, rows):
    return lax.dot_general(
        weight, rows, (((0,), (0,)), ((), ())), preferred_element_type=jnp.float32
    )


def causal_conv(values, taps, length):
    total = values.shape[1]
    position = jnp.arange(total, dtype=jnp.int32) % length
    shifted_one = jnp.pad(values, ((0, 0), (1, 0)))[:, :total]
    shifted_two = jnp.pad(values, ((0, 0), (2, 0)))[:, :total]
    shifted_one = jnp.where(position[None, :] >= 1, shifted_one, 0.0)
    shifted_two = jnp.where(position[None, :] >= 2, shifted_two, 0.0)
    return (
        taps[2][:, None] * values + taps[1][:, None] * shifted_one + taps[0][:, None] * shifted_two
    )


def gathered(
    residual,
    mixer_gain,
    value_weight,
    value_scale,
    input_gate_weight,
    input_gate_scale,
    output_gate_weight,
    output_gate_scale,
    conv_taps,
    conv_gain,
    mixer_out_weight,
    mixer_out_scale,
    channel_gain,
    gate_weight,
    gate_scale,
    up_weight,
    up_scale,
    down_weight,
    down_scale,
):
    own_rows = residual.shape[0]
    tokens = residual.shape[1]
    groups = lax.axis_size("tp")
    channels = value_weight.shape[1] * groups
    whole = lax.all_gather(residual, "tp", axis=0, tiled=True)
    normed = normalize(whole, mixer_gain)
    value = contract(
        lax.all_gather(value_weight.astype(jnp.bfloat16), "fs", axis=0, tiled=True), normed
    )
    in_gate = contract(
        lax.all_gather(input_gate_weight.astype(jnp.bfloat16), "fs", axis=0, tiled=True), normed
    )
    out_gate = contract(
        lax.all_gather(output_gate_weight.astype(jnp.bfloat16), "fs", axis=0, tiled=True), normed
    )
    value = value * value_scale[:, None]
    in_gate = in_gate * input_gate_scale[:, None]
    out_gate = out_gate * output_gate_scale[:, None]
    mixed = out_gate * causal_conv(in_gate * value, conv_taps, LEN)
    squares = lax.psum(jnp.sum(mixed * mixed, axis=0), "tp")
    conv_normed = (
        mixed * lax.rsqrt(squares / channels + epsilon)[None, :] * conv_gain[:, None]
    ).astype(jnp.bfloat16)
    out_full = lax.all_gather(mixer_out_weight.astype(jnp.bfloat16), "fs", axis=1, tiled=True)
    out_scale, down_scale_full = (
        lax.all_gather(mixer_out_scale, "fs", axis=0, tiled=True),
        lax.all_gather(down_scale, "fs", axis=0, tiled=True),
    )
    conv_all = lax.all_gather(conv_normed, "tp", axis=0, tiled=True)
    out_own = lax.all_to_all(out_full, "tp", split_axis=1, concat_axis=0, tiled=True)
    block_width = conv_normed.shape[0]
    weight_blocks = out_own.reshape(groups, block_width, own_rows)
    row_blocks = conv_all.reshape(groups, block_width, tokens)
    parts = lax.dot_general(
        weight_blocks, row_blocks, (((1,), (1,)), ((0,), (0,))), preferred_element_type=jnp.float32
    )
    own_scale = lax.dynamic_slice_in_dim(out_scale, lax.axis_index("tp") * own_rows, own_rows, 0)
    rounded = (parts * own_scale[None, :, None]).astype(jnp.bfloat16)
    total = jnp.sum(rounded.astype(jnp.float32), axis=0)
    after_own = (residual.astype(jnp.float32) + total).astype(jnp.bfloat16)
    after_whole = lax.all_gather(after_own, "tp", axis=0, tiled=True)
    normed_two = normalize(after_whole, channel_gain)
    gate_full, up_full = (
        lax.all_gather(gate_weight.astype(jnp.bfloat16), "fs", axis=0, tiled=True),
        lax.all_gather(up_weight.astype(jnp.bfloat16), "fs", axis=0, tiled=True),
    )
    gate = contract(gate_full, normed_two)
    upper = contract(up_full, normed_two)
    hidden = (jax.nn.silu(gate * gate_scale[:, None]) * (upper * up_scale[:, None])).astype(
        jnp.bfloat16
    )
    down_full = lax.all_gather(down_weight.astype(jnp.bfloat16), "fs", axis=1, tiled=True)
    total_two = lax.psum_scatter(
        (contract(down_full, hidden) * down_scale_full[:, None]).astype(jnp.bfloat16),
        "tp",
        scatter_dimension=0,
        tiled=True,
    ).astype(jnp.float32)
    return (after_own.astype(jnp.float32) + total_two).astype(jnp.bfloat16)


def flip(array, *axes):
    count = 2 ** len(axes)
    return lax.ppermute(array, axes, [(i, count - 1 - i) for i in range(count)])


def pick(array, index):
    return lax.dynamic_index_in_dim(array, index, 0, keepdims=False)


def in_order(index, own, other, axis):
    return jnp.where(
        index == 0,
        jnp.concatenate([own, other], axis=axis),
        jnp.concatenate([other, own], axis=axis),
    )


def feature_start(spot_ref, piece, y, width):
    rep, zh, zl = spot_ref[0], spot_ref[1], spot_ref[2]
    source = (zh ^ ((piece >> 1) & 1)) * 2 + (zl ^ (piece & 1))
    return (source * 2 + y) * 2 * width + (rep ^ (piece >> 2)) * width


def lay_out(spot_ref, pieces, full_ref):
    width = pieces[0].shape[1] // 2
    for index, piece in enumerate(pieces):
        for y in range(2):
            start = pl.multiple_of(feature_start(spot_ref, index, y, width), width)
            full_ref[:, pl.ds(start, width)] = piece[:, y * width : (y + 1) * width]


def tile_of(spot_ref, index):
    return (spot_ref[2] ^ (index >> 1)) * 2 + (spot_ref[3] ^ (index & 1))


def mix_kernel(spot_ref, *refs):
    rows, pieces = refs[:8], refs[8:16]
    taps_ref, mixed_ref, whole_ref, full_ref = refs[16:]
    lay_out(spot_ref, pieces, full_ref)
    half, tokens = rows[0].shape
    channels = mixed_ref.shape[0]
    position = lax.broadcasted_iota(jnp.int32, (channels, tokens), 1) % LEN
    for tile in range(4):
        total = jnp.zeros((3 * channels, tokens), jnp.float32)
        squares = jnp.zeros((1, tokens), jnp.float32)
        spot = pl.multiple_of(tile_of(spot_ref, tile) * tokens, tokens)
        for dx in range(2):
            block = rows[dx * 4 + tile][...]
            start = pl.multiple_of((spot_ref[4] ^ dx) * half, half)
            whole_ref[pl.ds(start, half), pl.ds(spot, tokens)] = block
            total = total + jnp.dot(
                full_ref[:, pl.ds(start, half)], block, preferred_element_type=jnp.float32
            )
            floats = block.astype(jnp.float32)
            squares = squares + jnp.sum(floats * floats, axis=0, keepdims=True)
        total = total * lax.rsqrt(squares / (2 * half) + epsilon)
        u = total[:channels] * total[channels : 2 * channels]
        one = jnp.where(position >= 1, pltpu.roll(u, 1, 1), 0.0)
        two = jnp.where(position >= 2, pltpu.roll(u, 2, 1), 0.0)
        conv = taps_ref[:, 2:3] * u + taps_ref[:, 1:2] * one + taps_ref[:, 0:1] * two
        mixed_ref[:, pl.ds(spot, tokens)] = (total[2 * channels :] * conv).astype(jnp.bfloat16)


def after_kernel(spot_ref, *refs):
    mixed, weights = refs[:8], refs[8:12]
    whole_ref, after_ref, own_ref, full_ref = refs[12:]
    channels, tokens = mixed[0].shape
    squares = jnp.zeros((1, tokens), jnp.float32)
    for index in range(8):
        block = mixed[index][...]
        spot = tile_of_channels(spot_ref, index & 3) * channels
        full_ref[index >> 2, pl.ds(pl.multiple_of(spot, channels), channels), :] = block
        floats = block.astype(jnp.float32)
        squares = squares + jnp.sum(floats * floats, axis=0, keepdims=True)
    scale = lax.rsqrt(squares / (8 * channels) + epsilon)
    width = weights[0].shape[1] // 2
    for index in range(8):
        rep, piece = index >> 2, index & 3
        part = jnp.dot(weights[2 * rep][piece], full_ref[0], preferred_element_type=jnp.float32)
        part = part + jnp.dot(
            weights[2 * rep + 1][piece], full_ref[1], preferred_element_type=jnp.float32
        )
        part = part * scale
        for y in range(2):
            start = pl.multiple_of(feature_start(spot_ref, index, y, width), width)
            total = whole_ref[pl.ds(start, width), :].astype(jnp.float32)
            total = total + part[y * width : (y + 1) * width]
            after_ref[pl.ds(start, width), :] = total.astype(jnp.bfloat16)

    @pl.when(pl.program_id(0) == spot_ref[2] * 2 + spot_ref[3])
    def _():
        half = own_ref.shape[0]
        start = pl.multiple_of(spot_ref[4] * half, half)
        own_ref[...] = after_ref[pl.ds(start, half), :]


def tile_of_channels(spot_ref, index):
    return (spot_ref[3] ^ (index & 1)) * 2 + (spot_ref[2] ^ (index >> 1))


def hidden_kernel(spot_ref, *refs):
    gates, ups = refs[:8], refs[8:16]
    after_ref, hidden_ref, gate_ref, up_ref = refs[16:]

    @pl.when(pl.program_id(0) == 0)
    def _():
        lay_out(spot_ref, gates, gate_ref)
        lay_out(spot_ref, ups, up_ref)

    rows = after_ref[...]
    floats = rows.astype(jnp.float32)
    squares = jnp.sum(floats * floats, axis=0, keepdims=True)
    scale = lax.rsqrt(squares / rows.shape[0] + epsilon)
    gate = jnp.dot(gate_ref[...], rows, preferred_element_type=jnp.float32) * scale
    upper = jnp.dot(up_ref[...], rows, preferred_element_type=jnp.float32) * scale
    hidden_ref[...] = (gate / (1.0 + jnp.exp(-gate)) * upper).astype(jnp.bfloat16)


def down_kernel(spot_ref, *refs):
    pieces, hidden_ref, outs, full_ref = refs[:8], refs[8], refs[9:17], refs[17]
    units, width = pieces[0].shape
    half, tokens = outs[0].shape
    for index, piece in enumerate(pieces):
        source = (spot_ref[1] ^ ((index >> 1) & 1)) * 2 + (spot_ref[2] ^ (index & 1))
        row = pl.multiple_of((spot_ref[0] ^ (index >> 2)) * units, units)
        column = pl.multiple_of(source * width, width)
        full_ref[pl.ds(row, units), pl.ds(column, width)] = piece[...]
    for tile in range(4):
        spot = pl.multiple_of(tile_of(spot_ref, tile) * tokens, tokens)
        hidden = hidden_ref[:, pl.ds(spot, tokens)]
        for dx in range(2):
            start = pl.multiple_of((spot_ref[4] ^ dx) * half, half)
            part = lax.dot_general(
                full_ref[:, pl.ds(start, half)],
                hidden,
                (((0,), (0,)), ((), ())),
                preferred_element_type=jnp.float32,
            )
            outs[dx * 4 + tile][...] = part.astype(jnp.bfloat16)


def whole_blocks(count):
    return [pl.BlockSpec(memory_space=pltpu.VMEM)] * count


def exchanged(
    residual,
    mixer_gain,
    value_weight,
    value_scale,
    input_gate_weight,
    input_gate_scale,
    output_gate_weight,
    output_gate_scale,
    conv_taps,
    conv_gain,
    mixer_out_weight,
    mixer_out_scale,
    channel_gain,
    gate_weight,
    gate_scale,
    up_weight,
    up_scale,
    down_weight,
    down_scale,
):
    spot = {axis: lax.axis_index(axis) for axis in ("rep", "zh", "zl", "y", "tp")}
    spots = jnp.stack([spot[axis] for axis in ("rep", "zh", "zl", "y", "tp")]).astype(jnp.int32)
    half, tokens = residual.shape
    depth = gate_weight.shape[0]
    own_depth = depth // 2
    features = 2 * half
    first = ((spot["zh"] * 2 + spot["zl"]) * 2 + spot["y"]) * depth + spot["rep"] * own_depth

    def own_rows(weight, gain, scale):
        rows = lax.dynamic_slice_in_dim(weight, spot["rep"] * own_depth, own_depth, 0)
        gains = lax.dynamic_slice_in_dim(gain, first, own_depth, 0)
        return (rows * gains[:, None] * scale[None, :]).astype(jnp.bfloat16).T

    def own_units(weight, gain, scale):
        return own_rows(weight, gain, scale).reshape(2, 2, weight.shape[1] // 4, own_depth)

    scalars = pl.BlockSpec(memory_space=pltpu.SMEM)

    rows = [residual, flip(residual, "y"), flip(residual, "zl")]
    rows.append(flip(rows[2], "y"))
    rows = rows + [flip(block, "tp") for block in rows]

    triple = jnp.concatenate(
        [
            own_units(weight, mixer_gain, scale)
            for weight, scale in (
                (value_weight, value_scale),
                (input_gate_weight, input_gate_scale),
                (output_gate_weight, output_gate_scale),
            )
        ],
        axis=2,
    )
    channels = value_weight.shape[1] // 4

    def spread_rows(blocks):
        keep = pick(blocks, spot["y"])
        got = flip(pick(blocks, 1 - spot["y"]), "y")
        zl = spot["zl"]
        mine = in_order(spot["y"], pick(keep, zl), pick(got, zl), 1)
        other = in_order(spot["y"], pick(keep, 1 - zl), pick(got, 1 - zl), 1)
        pieces = [mine, flip(other, "zl"), flip(mine, "zh"), flip(other, "zh", "zl")]
        return pieces + [flip(piece, "rep") for piece in pieces]

    projections = spread_rows(triple)
    own_taps = lax.dynamic_slice_in_dim(
        conv_taps, (spot["y"] * 2 + spot["zl"]) * channels, channels, 1
    ).T
    mixed, whole = pl.pallas_call(
        mix_kernel,
        out_shape=(
            jax.ShapeDtypeStruct((channels, 4 * tokens), jnp.bfloat16),
            jax.ShapeDtypeStruct((features, 4 * tokens), jnp.bfloat16),
        ),
        in_specs=[scalars] + whole_blocks(17),
        out_specs=tuple(whole_blocks(2)),
        scratch_shapes=[pltpu.VMEM((3 * channels, features), jnp.bfloat16)],
        name="mix",
    )(spots, *rows, *projections, own_taps)

    out_rows = lax.dynamic_slice_in_dim(mixer_out_weight, spot["rep"] * own_depth, own_depth, 1)
    out_scale = lax.dynamic_slice_in_dim(mixer_out_scale, spot["rep"] * own_depth, own_depth, 0)
    out_rows = (out_rows * conv_gain[:, None] * out_scale[None, :]).astype(jnp.bfloat16).T
    out_pair = in_order(spot["y"], out_rows, flip(out_rows, "y"), 0)
    out_own = jnp.stack(
        [out_pair, flip(out_pair, "zl"), flip(out_pair, "zh"), flip(out_pair, "zh", "zl")]
    )
    out_weights = [out_own, flip(out_own, "tp")]
    out_weights = out_weights + [flip(block, "rep") for block in out_weights]

    mixes = [mixed, flip(mixed, "y"), flip(mixed, "zl"), flip(mixed, "zl", "y")]
    mixes = mixes + [
        flip(mixed, "tp"),
        flip(mixed, "y", "tp"),
        flip(mixed, "zl", "tp"),
        flip(mixed, "zl", "y", "tp"),
    ]
    tile = lambda shape: pl.BlockSpec(shape, lambda i: (0, i))
    fixed = lambda shape: pl.BlockSpec(shape, lambda i: (0,) * len(shape))
    after, after_own = pl.pallas_call(
        after_kernel,
        grid=(4,),
        out_shape=(
            jax.ShapeDtypeStruct((features, 4 * tokens), jnp.bfloat16),
            jax.ShapeDtypeStruct((half, tokens), jnp.bfloat16),
        ),
        in_specs=[scalars]
        + [tile((channels, tokens))] * 8
        + [fixed(out_own.shape)] * 4
        + [tile((features, tokens))],
        out_specs=(tile((features, tokens)), fixed((half, tokens))),
        scratch_shapes=[pltpu.VMEM((2, 4 * channels, tokens), jnp.bfloat16)],
        name="after",
    )(spots, *mixes, *out_weights, whole)

    gates = spread_rows(own_units(gate_weight, channel_gain, gate_scale))
    ups = spread_rows(own_units(up_weight, channel_gain, up_scale))
    units = gate_weight.shape[1] // 4
    hidden = pl.pallas_call(
        hidden_kernel,
        grid=(4,),
        out_shape=jax.ShapeDtypeStruct((units, 4 * tokens), jnp.bfloat16),
        in_specs=[scalars] + [fixed(gates[0].shape)] * 16 + [tile((features, tokens))],
        out_specs=tile((units, tokens)),
        scratch_shapes=[pltpu.VMEM((units, features), jnp.bfloat16)] * 2,
        name="hidden",
    )(spots, *gates, *ups, after)

    downs = (down_weight * down_scale[None, :]).reshape(2, 2, 2, units // 2, depth)
    downs = lax.dynamic_index_in_dim(downs, spot["rep"], 2, keepdims=False).astype(jnp.bfloat16)
    down_pieces = spread_rows(downs)
    parts = pl.pallas_call(
        down_kernel,
        out_shape=(jax.ShapeDtypeStruct((half, tokens), jnp.bfloat16),) * 8,
        in_specs=[scalars] + whole_blocks(9),
        out_specs=tuple(whole_blocks(8)),
        scratch_shapes=[pltpu.VMEM((units, features), jnp.bfloat16)],
        name="down",
    )(spots, *down_pieces, hidden)
    others = [
        flip(parts[7], "zl", "y", "tp"),
        flip(parts[6], "zl", "tp"),
        flip(parts[5], "y", "tp"),
        flip(parts[4], "tp"),
        flip(parts[3], "zl", "y"),
        flip(parts[2], "zl"),
        flip(parts[1], "y"),
    ]
    total = parts[0].astype(jnp.float32)
    for other in others:
        total = total + other.astype(jnp.float32)
    return (after_own.astype(jnp.float32) + total).astype(jnp.bfloat16)


def solution(mesh):
    sizes = dict(mesh.shape)
    if sizes == {"rep": 2, "fs": 8, "tp": 2}:
        grid = Mesh(mesh.devices.reshape(2, 2, 2, 2, 2), ("rep", "zh", "zl", "y", "tp"))
        fs, step = ("zh", "zl", "y"), exchanged
    else:
        grid, fs, step = mesh, ("fs",), gathered
    own = P("tp", ("rep",) + fs)
    placed = (
        own,
        P(),
        P(fs, "tp"),
        P("tp"),
        P(fs, "tp"),
        P("tp"),
        P(fs, "tp"),
        P("tp"),
        P(None, "tp"),
        P("tp"),
        P("tp", fs),
        P(fs),
        P(),
        P(fs, "tp"),
        P("tp"),
        P(fs, "tp"),
        P("tp"),
        P("tp", fs),
        P(fs),
    )
    return jax.shard_map(step, mesh=grid, in_specs=placed, out_specs=own, check_vma=False)
```

```python
import jax
import jax.numpy as jnp
from jax import lax
from jax.experimental import pallas as pl
from jax.experimental.pallas import tpu as pltpu
from jax.sharding import Mesh
from jax.sharding import PartitionSpec as P

LEN = 128


epsilon = 1e-06


def normalize(values, gain):
    floats = values.astype(jnp.float32)
    mean = jnp.mean(floats * floats, axis=0, keepdims=True)
    return (floats * lax.rsqrt(mean + epsilon) * gain[:, None]).astype(jnp.bfloat16)


def contract(weight, rows):
    return lax.dot_general(
        weight, rows, (((0,), (0,)), ((), ())), preferred_element_type=jnp.float32
    )


def causal_conv(values, taps, length):
    total = values.shape[1]
    position = jnp.arange(total, dtype=jnp.int32) % length
    shifted_one = jnp.pad(values, ((0, 0), (1, 0)))[:, :total]
    shifted_two = jnp.pad(values, ((0, 0), (2, 0)))[:, :total]
    shifted_one = jnp.where(position[None, :] >= 1, shifted_one, 0.0)
    shifted_two = jnp.where(position[None, :] >= 2, shifted_two, 0.0)
    return (
        taps[2][:, None] * values + taps[1][:, None] * shifted_one + taps[0][:, None] * shifted_two
    )


def gathered(
    residual,
    mixer_gain,
    value_weight,
    value_scale,
    input_gate_weight,
    input_gate_scale,
    output_gate_weight,
    output_gate_scale,
    conv_taps,
    conv_gain,
    mixer_out_weight,
    mixer_out_scale,
    channel_gain,
    gate_weight,
    gate_scale,
    up_weight,
    up_scale,
    down_weight,
    down_scale,
):
    own_rows = residual.shape[0]
    tokens = residual.shape[1]
    groups = lax.axis_size("tp")
    channels = value_weight.shape[1] * groups
    whole = lax.all_gather(residual, "tp", axis=0, tiled=True)
    normed = normalize(whole, mixer_gain)
    value = contract(
        lax.all_gather(value_weight.astype(jnp.bfloat16), "fs", axis=0, tiled=True), normed
    )
    in_gate = contract(
        lax.all_gather(input_gate_weight.astype(jnp.bfloat16), "fs", axis=0, tiled=True), normed
    )
    out_gate = contract(
        lax.all_gather(output_gate_weight.astype(jnp.bfloat16), "fs", axis=0, tiled=True), normed
    )
    value = value * value_scale[:, None]
    in_gate = in_gate * input_gate_scale[:, None]
    out_gate = out_gate * output_gate_scale[:, None]
    mixed = out_gate * causal_conv(in_gate * value, conv_taps, LEN)
    squares = lax.psum(jnp.sum(mixed * mixed, axis=0), "tp")
    conv_normed = (
        mixed * lax.rsqrt(squares / channels + epsilon)[None, :] * conv_gain[:, None]
    ).astype(jnp.bfloat16)
    out_full = lax.all_gather(mixer_out_weight.astype(jnp.bfloat16), "fs", axis=1, tiled=True)
    out_scale, down_scale_full = (
        lax.all_gather(mixer_out_scale, "fs", axis=0, tiled=True),
        lax.all_gather(down_scale, "fs", axis=0, tiled=True),
    )
    conv_all = lax.all_gather(conv_normed, "tp", axis=0, tiled=True)
    out_own = lax.all_to_all(out_full, "tp", split_axis=1, concat_axis=0, tiled=True)
    block_width = conv_normed.shape[0]
    weight_blocks = out_own.reshape(groups, block_width, own_rows)
    row_blocks = conv_all.reshape(groups, block_width, tokens)
    parts = lax.dot_general(
        weight_blocks, row_blocks, (((1,), (1,)), ((0,), (0,))), preferred_element_type=jnp.float32
    )
    own_scale = lax.dynamic_slice_in_dim(out_scale, lax.axis_index("tp") * own_rows, own_rows, 0)
    rounded = (parts * own_scale[None, :, None]).astype(jnp.bfloat16)
    total = jnp.sum(rounded.astype(jnp.float32), axis=0)
    after_own = (residual.astype(jnp.float32) + total).astype(jnp.bfloat16)
    after_whole = lax.all_gather(after_own, "tp", axis=0, tiled=True)
    normed_two = normalize(after_whole, channel_gain)
    gate_full, up_full = (
        lax.all_gather(gate_weight.astype(jnp.bfloat16), "fs", axis=0, tiled=True),
        lax.all_gather(up_weight.astype(jnp.bfloat16), "fs", axis=0, tiled=True),
    )
    gate = contract(gate_full, normed_two)
    upper = contract(up_full, normed_two)
    hidden = (jax.nn.silu(gate * gate_scale[:, None]) * (upper * up_scale[:, None])).astype(
        jnp.bfloat16
    )
    down_full = lax.all_gather(down_weight.astype(jnp.bfloat16), "fs", axis=1, tiled=True)
    total_two = lax.psum_scatter(
        (contract(down_full, hidden) * down_scale_full[:, None]).astype(jnp.bfloat16),
        "tp",
        scatter_dimension=0,
        tiled=True,
    ).astype(jnp.float32)
    return (after_own.astype(jnp.float32) + total_two).astype(jnp.bfloat16)


def flip(array, *axes):
    count = 2 ** len(axes)
    return lax.ppermute(array, axes, [(i, count - 1 - i) for i in range(count)])


def feature_block(spot_ref, piece, dy):
    zh, zl, y = spot_ref[1], spot_ref[2], spot_ref[3]
    return ((zh ^ (piece >> 1)) * 2 + (zl ^ (piece & 1))) * 2 + (y ^ dy)


def lay_out(spot_ref, index, piece, full_ref):
    width = piece.shape[1]
    start = feature_block(spot_ref, index & 3, index >> 2) * width
    full_ref[:, pl.ds(pl.multiple_of(start, width), width)] = piece


def tile_of(spot_ref, index):
    return (spot_ref[2] ^ (index >> 1)) * 2 + (spot_ref[0] ^ (index & 1))


def channels_of(spot_ref, index):
    return (spot_ref[0] ^ (index & 1)) * 2 + (spot_ref[2] ^ (index >> 1))


def own_row(array, row):
    rows = lax.broadcasted_iota(jnp.int32, array.shape, 0)
    return jnp.sum(jnp.where(rows == row, array, 0.0), axis=0, keepdims=True)


def turn(spot_ref, weight_ref, scale_ref, gain, turned_ref):
    lanes = scale_ref.shape[1]
    scales = scale_ref[...]
    count = weight_ref.shape[1] // lanes
    for index in range(count):
        place = slice(index * lanes, (index + 1) * lanes)
        scaled = weight_ref[:, place] * own_row(scales, spot_ref[0] * count + index)
        turned_ref[place, :] = (scaled.T * gain).astype(jnp.bfloat16)


def own_gain(spot_ref, gain_ref):
    block, gains = feature_block(spot_ref, 0, 0), gain_ref[...]
    return jnp.concatenate([own_row(gains, 2 * block), own_row(gains, 2 * block + 1)], axis=1)


def small_kernel(spot_ref, *refs):
    weights, scales, gain_ref = refs[:3], refs[3:6], refs[6]
    out_ref, conv_gain_ref, out_scale_ref, mine_ref, other_ref, turned_ref = refs[7:]
    rep, zl = spot_ref[0], spot_ref[2]
    lanes = weights[0].shape[1]
    channels = lanes // 2
    gain = own_gain(spot_ref, gain_ref)
    for index in range(3):
        turn(spot_ref, weights[index], scales[index], gain, turned_ref)
        for target, dl, place in ((mine_ref, 0, 0), (other_ref, 1, lanes)):
            start = pl.multiple_of((zl ^ dl) * channels, channels)
            place = place + index * channels
            target[place : place + channels, :] = turned_ref[pl.ds(start, channels), :]
    scale = own_row(out_scale_ref[...], rep)
    for index in range(2):
        place = slice(index * lanes, (index + 1) * lanes)
        turned = (out_ref[place, :] * scale).T * own_row(conv_gain_ref[...], index)
        rows = turned.astype(jnp.bfloat16)
        mine_ref[3 * channels :, place] = rows
        other_ref[:lanes, place] = rows


def pair_kernel(spot_ref, *refs):
    weights, scales, gain_ref, targets, turned_ref = refs[:2], refs[2:4], refs[4], refs[5:9], refs[9]
    gain = own_gain(spot_ref, gain_ref)
    for index in range(2):
        turn(spot_ref, weights[index], scales[index], gain, turned_ref)
        units = targets[0].shape[0]
        for dl in range(2):
            start = pl.multiple_of((spot_ref[2] ^ dl) * units, 16)
            targets[2 * index + dl][...] = turned_ref[pl.ds(start, units), :]


def last_kernel(spot_ref, weight_ref, scale_ref, *targets):
    units, width = targets[0].shape
    for chunk in range(2):
        scale = own_row(scale_ref[...], chunk)
        for dl in range(2):
            start = pl.multiple_of((spot_ref[2] ^ dl) * units, 16)
            rows = weight_ref[pl.ds(start, units), chunk * width : (chunk + 1) * width]
            targets[2 * chunk + dl][...] = (rows * scale).astype(jnp.bfloat16)


def mix_kernel(spot_ref, *refs):
    rows, own_ref, twin_ref = refs[:8], refs[8], refs[9]
    taps_ref, mixed_ref, whole_ref, full_ref = refs[10:]
    half, tokens = rows[0].shape
    channels = mixed_ref.shape[0]
    for index in range(4):
        lay_out(spot_ref, index, own_ref[index], full_ref)
        lay_out(spot_ref, index + 4, twin_ref[index], full_ref)
    position = lax.broadcasted_iota(jnp.int32, (channels, tokens), 1) % LEN
    for tile in range(4):
        total = jnp.zeros((3 * channels, tokens), jnp.float32)
        squares = jnp.zeros((1, tokens), jnp.float32)
        spot = pl.multiple_of(tile_of(spot_ref, tile) * tokens, tokens)
        for dx in range(2):
            block = rows[dx * 4 + tile][...]
            start = pl.multiple_of((spot_ref[4] ^ dx) * half, half)
            whole_ref[pl.ds(start, half), pl.ds(spot, tokens)] = block
            total = total + jnp.dot(
                full_ref[:, pl.ds(start, half)], block, preferred_element_type=jnp.float32
            )
            floats = block.astype(jnp.float32)
            squares = squares + jnp.sum(floats * floats, axis=0, keepdims=True)
        total = total * lax.rsqrt(squares / (2 * half) + epsilon)
        u = total[:channels] * total[channels : 2 * channels]
        one = jnp.where(position >= 1, pltpu.roll(u, 1, 1), 0.0)
        two = jnp.where(position >= 2, pltpu.roll(u, 2, 1), 0.0)
        conv = taps_ref[:, 2:3] * u + taps_ref[:, 1:2] * one + taps_ref[:, 0:1] * two
        mixed_ref[:, pl.ds(spot, tokens)] = (total[2 * channels :] * conv).astype(jnp.bfloat16)


def after_kernel(spot_ref, *refs):
    mixed, own_ref, other_ref, twin_ref = refs[:2], *refs[2:5]
    whole_ref, after_ref, kept_ref, full_ref, weight_ref = refs[5:]
    channels, tokens = mixed[0].shape[1:]
    width = weight_ref.shape[0] // 16

    @pl.when(pl.program_id(0) == 0)
    def _():
        for piece in range(4):
            for dy in range(2):
                block = feature_block(spot_ref, piece, dy)
                for dr in range(2):
                    start = pl.multiple_of((block * 2 + (spot_ref[0] ^ dr)) * width, width)
                    for dx in range(2):
                        part = (own_ref, other_ref)[dx][dy, piece]
                        if dr:
                            part = twin_ref[dx, dy, piece]
                        place = slice(dx * 2 * width, (dx + 1) * 2 * width)
                        weight_ref[pl.ds(start, width), place] = part

    squares = jnp.zeros((1, tokens), jnp.float32)
    for dr in range(2):
        for index in range(4):
            block = mixed[dr][index]
            spot = channels_of(spot_ref, (index & 1) * 2 + dr)
            spot = ((index >> 1) * 4 + spot) * channels
            full_ref[pl.ds(pl.multiple_of(spot, channels), channels), :] = block
            floats = block.astype(jnp.float32)
            squares = squares + jnp.sum(floats * floats, axis=0, keepdims=True)
    scale = lax.rsqrt(squares / (8 * channels) + epsilon)
    part = jnp.dot(weight_ref[...], full_ref[...], preferred_element_type=jnp.float32)
    total = whole_ref[...].astype(jnp.float32) + part * scale
    after_ref[...] = total.astype(jnp.bfloat16)

    @pl.when(pl.program_id(0) == tile_of(spot_ref, 0))
    def _():
        half = kept_ref.shape[0]
        start = pl.multiple_of(spot_ref[4] * half, half)
        kept_ref[...] = after_ref[pl.ds(start, half), :]


def norm_scale(rows):
    floats = rows.astype(jnp.float32)
    squares = jnp.sum(floats * floats, axis=0, keepdims=True)
    return lax.rsqrt(squares / rows.shape[0] + epsilon)


def gate_kernel(spot_ref, *refs):
    pieces, after_ref, active_ref, gate_ref = refs[:8], *refs[8:]

    @pl.when(pl.program_id(0) == 0)
    def _():
        for index in range(8):
            lay_out(spot_ref, index, pieces[index][...], gate_ref)

    rows = after_ref[...]
    gate = jnp.dot(gate_ref[...], rows, preferred_element_type=jnp.float32) * norm_scale(rows)
    active_ref[...] = gate / (1.0 + jnp.exp(-gate))


def hidden_kernel(spot_ref, *refs):
    pieces, after_ref, active_ref, hidden_ref, up_ref = refs[:8], *refs[8:]

    @pl.when(pl.program_id(0) == 0)
    def _():
        for index in range(8):
            lay_out(spot_ref, index, pieces[index][...], up_ref)

    rows = after_ref[...]
    upper = jnp.dot(up_ref[...], rows, preferred_element_type=jnp.float32) * norm_scale(rows)
    hidden_ref[...] = (active_ref[...] * upper).astype(jnp.bfloat16)


def down_kernel(spot_ref, *refs):
    pieces, hidden_ref, outs, full_ref = refs[:8], refs[8], refs[9:11], refs[11]
    half, tokens = outs[0].shape[1:]
    for index in range(8):
        lay_out(spot_ref, index, pieces[index][...], full_ref)
    for dr in (1, 0):
        for dl in range(2):
            spot = pl.multiple_of(tile_of(spot_ref, dl * 2 + dr) * tokens, tokens)
            hidden = hidden_ref[:, pl.ds(spot, tokens)]
            for dx in range(2):
                start = pl.multiple_of((spot_ref[4] ^ dx) * half, half)
                part = lax.dot_general(
                    full_ref[:, pl.ds(start, half)],
                    hidden,
                    (((0,), (0,)), ((), ())),
                    preferred_element_type=jnp.float32,
                )
                outs[dr][dx * 2 + dl] = part.astype(jnp.bfloat16)


def shaped(*shape):
    return jax.ShapeDtypeStruct(shape, jnp.bfloat16)


def whole_blocks(count):
    return [pl.BlockSpec(memory_space=pltpu.VMEM)] * count


def exchanged(
    residual,
    mixer_gain,
    value_weight,
    value_scale,
    input_gate_weight,
    input_gate_scale,
    output_gate_weight,
    output_gate_scale,
    conv_taps,
    conv_gain,
    mixer_out_weight,
    mixer_out_scale,
    channel_gain,
    gate_weight,
    gate_scale,
    up_weight,
    up_scale,
    down_weight,
    down_scale,
):
    axes = ("rep", "zh", "zl", "y", "tp")
    spots = jnp.stack([lax.axis_index(axis) for axis in axes]).astype(jnp.int32)
    half, tokens = residual.shape
    depth = gate_weight.shape[0]
    lanes = depth // 2
    features = 2 * half
    channels = value_weight.shape[1] // 4
    units = gate_weight.shape[1] // 4
    scalars = pl.BlockSpec(memory_space=pltpu.SMEM)
    tile = lambda shape: pl.BlockSpec(shape, lambda i: (0,) * (len(shape) - 1) + (i,))
    fixed = lambda shape: pl.BlockSpec(shape, lambda i: (0,) * len(shape))

    def by_lane(array):
        return array.reshape(-1, lanes)

    def prepare(kernel, operands, half_columns, half_rows, outs, scratch):
        def block(operand):
            if any(operand is weight for weight in half_columns):
                shape = (operand.shape[0], operand.shape[1] // 2)
                return pl.BlockSpec(shape, lambda i, spot_ref: (0, spot_ref[0]))
            if any(operand is weight for weight in half_rows):
                shape = (operand.shape[0] // 2, operand.shape[1])
                return pl.BlockSpec(shape, lambda i, spot_ref: (spot_ref[0], 0))
            return pl.BlockSpec(operand.shape, lambda i, spot_ref: (0, 0))

        return pl.pallas_call(
            kernel,
            out_shape=tuple(shaped(*shape) for shape in outs),
            grid_spec=pltpu.PrefetchScalarGridSpec(
                num_scalar_prefetch=1,
                grid=(1,),
                in_specs=[block(operand) for operand in operands],
                out_specs=tuple(pl.BlockSpec(shape, lambda i, spot_ref: (0, 0)) for shape in outs),
                scratch_shapes=scratch,
            ),
        )(spots, *operands)

    def run(kernel, operands, in_specs, outs, out_specs, scratch, grid=(4,)):
        return pl.pallas_call(
            kernel,
            grid=grid,
            out_shape=outs,
            in_specs=[scalars] + in_specs,
            out_specs=out_specs,
            scratch_shapes=scratch,
        )(spots, *operands)

    def over_z(mine, other):
        return [mine, flip(other, "zl"), flip(mine, "zh"), flip(other, "zh", "zl")]

    def over_y(pieces):
        return pieces + [flip(piece, "y") for piece in pieces]

    rows_zl = flip(residual, "zl")
    rows_tp = flip(residual, "tp")
    rows_both = flip(rows_zl, "tp")
    rows = []
    for block in (residual, rows_zl, rows_tp, rows_both):
        rows = rows + [block, flip(block, "rep")]

    small = (value_weight, input_gate_weight, output_gate_weight)
    mine, other = prepare(
        small_kernel,
        small
        + (by_lane(value_scale), by_lane(input_gate_scale), by_lane(output_gate_scale))
        + (by_lane(mixer_gain), mixer_out_weight, by_lane(conv_gain), by_lane(mixer_out_scale)),
        small + (mixer_out_weight,),
        (),
        [(3 * channels + lanes, depth)] * 2,
        [pltpu.VMEM((lanes, depth), jnp.bfloat16)],
    )
    small_pieces = over_z(mine, other)

    pair = (gate_weight, up_weight)
    pairs = prepare(
        pair_kernel,
        pair + (by_lane(gate_scale), by_lane(up_scale), by_lane(channel_gain)),
        pair,
        (),
        [(units, depth)] * 4,
        [pltpu.VMEM((2 * units, depth), jnp.bfloat16)],
    )
    gates = over_y(over_z(pairs[0], pairs[1]))
    ups = over_y(over_z(pairs[2], pairs[3]))
    downs = prepare(
        last_kernel,
        (down_weight, by_lane(down_scale)),
        (),
        (down_weight,),
        [(units, lanes)] * 4,
        [],
    )
    lasts = over_y(over_z(downs[0], downs[1]))
    lasts = lasts + over_y(over_z(downs[2], downs[3]))
    small_pieces, _ = lax.optimization_barrier((small_pieces, downs[0]))

    places = [lanes * (piece & 1) for piece in range(4)]
    projections = jnp.stack(
        [block[place : place + 3 * channels] for block, place in zip(small_pieces, places)]
    )
    other_projections = flip(projections, "y")
    places = [3 * channels * (1 - (piece & 1)) for piece in range(4)]
    own_out = jnp.stack([block[place : place + lanes] for block, place in zip(small_pieces, places)])
    same_out = flip(own_out, "y")
    place = (lax.axis_index("rep") * 2 + lax.axis_index("zl")) * channels
    own_taps = lax.dynamic_slice_in_dim(conv_taps, place, channels, 1).T
    mixed, whole = run(
        mix_kernel,
        rows[:4] + rows[4:] + [projections, other_projections, own_taps],
        whole_blocks(11),
        (shaped(channels, 4 * tokens), shaped(features, 4 * tokens)),
        tuple(whole_blocks(2)),
        [pltpu.VMEM((3 * channels, features), jnp.bfloat16)],
        grid=(),
    )
    same_out, mixed = lax.optimization_barrier((same_out, mixed))
    out_blocks = jnp.stack([own_out, same_out])
    out_other = flip(out_blocks, "tp")
    out_twin = flip(jnp.stack([out_blocks, out_other]), "rep")
    mixes = jnp.stack([mixed, flip(mixed, "zl"), flip(mixed, "tp"), flip(mixed, "zl", "tp")])
    twin_mixes = flip(mixes, "rep")
    after, after_own = run(
        after_kernel,
        [mixes, twin_mixes, out_blocks, out_other, out_twin, whole],
        [tile((4, channels, tokens))] * 2
        + [fixed(block.shape) for block in (out_blocks, out_other, out_twin)]
        + [tile((features, tokens))],
        (shaped(features, 4 * tokens), shaped(half, tokens)),
        (tile((features, tokens)), fixed((half, tokens))),
        [
            pltpu.VMEM((8 * channels, tokens), jnp.bfloat16),
            pltpu.VMEM((features, 8 * channels), jnp.bfloat16),
        ],
    )

    blocks = [fixed((units, depth))] * 8 + [tile((features, tokens))]
    scratch = [pltpu.VMEM((units, features), jnp.bfloat16)]
    active = run(
        gate_kernel,
        gates + [after],
        blocks,
        jax.ShapeDtypeStruct((units, 4 * tokens), jnp.float32),
        tile((units, tokens)),
        scratch,
    )
    hidden = run(
        hidden_kernel,
        ups + [after, active],
        blocks + [tile((units, tokens))],
        shaped(units, 4 * tokens),
        tile((units, tokens)),
        scratch,
    )
    totals = []
    for chunk in range(2):
        kept, sent = run(
            down_kernel,
            lasts[8 * chunk :][:8] + [hidden],
            whole_blocks(9),
            (shaped(4, half // 2, tokens),) * 2,
            tuple(whole_blocks(2)),
            [pltpu.VMEM((units, half), jnp.bfloat16)],
            grid=(),
        )
        got = flip(sent, "rep")
        sums = kept.astype(jnp.float32) + got.astype(jnp.float32)
        own = after_own.reshape(-1, 2, lanes, tokens)[:, chunk].reshape(-1, tokens)
        total = own.astype(jnp.float32) + sums[0]
        for index, way in ((3, ("zl", "tp")), (2, ("tp",)), (1, ("zl",))):
            part = flip(sums[index].astype(jnp.bfloat16), *way)
            total = total + part.astype(jnp.float32)
        totals.append(total.astype(jnp.bfloat16).reshape(-1, lanes, tokens))
    return jnp.stack(totals, axis=1).reshape(half, tokens)


def solution(mesh):
    sizes = dict(mesh.shape)
    if sizes == {"rep": 2, "fs": 8, "tp": 2}:
        grid = Mesh(mesh.devices.reshape(2, 2, 2, 2, 2), ("rep", "zh", "zl", "y", "tp"))
        fs, step = ("zh", "zl", "y"), exchanged
    else:
        grid, fs, step = mesh, ("fs",), gathered
    own = P("tp", ("rep",) + fs)
    placed = (
        own,
        P(),
        P(fs, "tp"),
        P("tp"),
        P(fs, "tp"),
        P("tp"),
        P(fs, "tp"),
        P("tp"),
        P(None, "tp"),
        P("tp"),
        P("tp", fs),
        P(fs),
        P(),
        P(fs, "tp"),
        P("tp"),
        P(fs, "tp"),
        P("tp"),
        P("tp", fs),
        P(fs),
    )
    step = jax.shard_map(step, mesh=grid, in_specs=placed, out_specs=own, check_vma=False)
    return step
```

```python
import jax
import jax.numpy as jnp
from jax import lax
from jax.experimental import pallas as pl
from jax.experimental.pallas import tpu as pltpu
from jax.sharding import Mesh
from jax.sharding import PartitionSpec as P

LEN = 128


epsilon = 1e-06


def normalize(values, gain):
    floats = values.astype(jnp.float32)
    mean = jnp.mean(floats * floats, axis=0, keepdims=True)
    return (floats * lax.rsqrt(mean + epsilon) * gain[:, None]).astype(jnp.bfloat16)


def contract(weight, rows):
    return lax.dot_general(
        weight, rows, (((0,), (0,)), ((), ())), preferred_element_type=jnp.float32
    )


def causal_conv(values, taps, length):
    total = values.shape[1]
    position = jnp.arange(total, dtype=jnp.int32) % length
    shifted_one = jnp.pad(values, ((0, 0), (1, 0)))[:, :total]
    shifted_two = jnp.pad(values, ((0, 0), (2, 0)))[:, :total]
    shifted_one = jnp.where(position[None, :] >= 1, shifted_one, 0.0)
    shifted_two = jnp.where(position[None, :] >= 2, shifted_two, 0.0)
    return (
        taps[2][:, None] * values + taps[1][:, None] * shifted_one + taps[0][:, None] * shifted_two
    )


def gathered(
    residual,
    mixer_gain,
    value_weight,
    value_scale,
    input_gate_weight,
    input_gate_scale,
    output_gate_weight,
    output_gate_scale,
    conv_taps,
    conv_gain,
    mixer_out_weight,
    mixer_out_scale,
    channel_gain,
    gate_weight,
    gate_scale,
    up_weight,
    up_scale,
    down_weight,
    down_scale,
):
    own_rows = residual.shape[0]
    tokens = residual.shape[1]
    groups = lax.axis_size("tp")
    channels = value_weight.shape[1] * groups
    whole = lax.all_gather(residual, "tp", axis=0, tiled=True)
    normed = normalize(whole, mixer_gain)
    value = contract(
        lax.all_gather(value_weight.astype(jnp.bfloat16), "fs", axis=0, tiled=True), normed
    )
    in_gate = contract(
        lax.all_gather(input_gate_weight.astype(jnp.bfloat16), "fs", axis=0, tiled=True), normed
    )
    out_gate = contract(
        lax.all_gather(output_gate_weight.astype(jnp.bfloat16), "fs", axis=0, tiled=True), normed
    )
    value = value * value_scale[:, None]
    in_gate = in_gate * input_gate_scale[:, None]
    out_gate = out_gate * output_gate_scale[:, None]
    mixed = out_gate * causal_conv(in_gate * value, conv_taps, LEN)
    squares = lax.psum(jnp.sum(mixed * mixed, axis=0), "tp")
    conv_normed = (
        mixed * lax.rsqrt(squares / channels + epsilon)[None, :] * conv_gain[:, None]
    ).astype(jnp.bfloat16)
    out_full = lax.all_gather(mixer_out_weight.astype(jnp.bfloat16), "fs", axis=1, tiled=True)
    out_scale, down_scale_full = (
        lax.all_gather(mixer_out_scale, "fs", axis=0, tiled=True),
        lax.all_gather(down_scale, "fs", axis=0, tiled=True),
    )
    conv_all = lax.all_gather(conv_normed, "tp", axis=0, tiled=True)
    out_own = lax.all_to_all(out_full, "tp", split_axis=1, concat_axis=0, tiled=True)
    block_width = conv_normed.shape[0]
    weight_blocks = out_own.reshape(groups, block_width, own_rows)
    row_blocks = conv_all.reshape(groups, block_width, tokens)
    parts = lax.dot_general(
        weight_blocks, row_blocks, (((1,), (1,)), ((0,), (0,))), preferred_element_type=jnp.float32
    )
    own_scale = lax.dynamic_slice_in_dim(out_scale, lax.axis_index("tp") * own_rows, own_rows, 0)
    rounded = (parts * own_scale[None, :, None]).astype(jnp.bfloat16)
    total = jnp.sum(rounded.astype(jnp.float32), axis=0)
    after_own = (residual.astype(jnp.float32) + total).astype(jnp.bfloat16)
    after_whole = lax.all_gather(after_own, "tp", axis=0, tiled=True)
    normed_two = normalize(after_whole, channel_gain)
    gate_full, up_full = (
        lax.all_gather(gate_weight.astype(jnp.bfloat16), "fs", axis=0, tiled=True),
        lax.all_gather(up_weight.astype(jnp.bfloat16), "fs", axis=0, tiled=True),
    )
    gate = contract(gate_full, normed_two)
    upper = contract(up_full, normed_two)
    hidden = (jax.nn.silu(gate * gate_scale[:, None]) * (upper * up_scale[:, None])).astype(
        jnp.bfloat16
    )
    down_full = lax.all_gather(down_weight.astype(jnp.bfloat16), "fs", axis=1, tiled=True)
    total_two = lax.psum_scatter(
        (contract(down_full, hidden) * down_scale_full[:, None]).astype(jnp.bfloat16),
        "tp",
        scatter_dimension=0,
        tiled=True,
    ).astype(jnp.float32)
    return (after_own.astype(jnp.float32) + total_two).astype(jnp.bfloat16)


def flip(array, *axes):
    count = 2 ** len(axes)
    return lax.ppermute(array, axes, [(i, count - 1 - i) for i in range(count)])


def feature_block(spot_ref, piece, dy):
    zh, zl, y = spot_ref[1], spot_ref[2], spot_ref[3]
    return ((zh ^ (piece >> 1)) * 2 + (zl ^ (piece & 1))) * 2 + (y ^ dy)


def lay_out(spot_ref, index, piece, full_ref):
    width = piece.shape[1]
    start = feature_block(spot_ref, index & 3, index >> 2) * width
    full_ref[:, pl.ds(pl.multiple_of(start, width), width)] = piece


def tile_of(spot_ref, index):
    return (spot_ref[2] ^ (index >> 1)) * 2 + (spot_ref[0] ^ (index & 1))


def channels_of(spot_ref, index):
    return (spot_ref[0] ^ (index & 1)) * 2 + (spot_ref[2] ^ (index >> 1))


def own_row(array, row):
    rows = lax.broadcasted_iota(jnp.int32, array.shape, 0)
    return jnp.sum(jnp.where(rows == row, array, 0.0), axis=0, keepdims=True)


def turn(spot_ref, weight_ref, scale_ref, gain, turned_ref):
    lanes = scale_ref.shape[1]
    scales = scale_ref[...]
    count = weight_ref.shape[1] // lanes
    for index in range(count):
        place = slice(index * lanes, (index + 1) * lanes)
        scaled = weight_ref[:, place] * own_row(scales, spot_ref[0] * count + index)
        turned_ref[place, :] = (scaled.T * gain).astype(jnp.bfloat16)


def own_gain(spot_ref, gain_ref):
    block, gains = feature_block(spot_ref, 0, 0), gain_ref[...]
    return jnp.concatenate([own_row(gains, 2 * block), own_row(gains, 2 * block + 1)], axis=1)


def small_kernel(spot_ref, *refs):
    weights, scales, gain_ref = refs[:3], refs[3:6], refs[6]
    out_ref, conv_gain_ref, out_scale_ref, mine_ref, other_ref, turned_ref = refs[7:]
    rep, zl = spot_ref[0], spot_ref[2]
    lanes = weights[0].shape[1]
    channels = lanes // 2
    gain = own_gain(spot_ref, gain_ref)
    for index in range(3):
        turn(spot_ref, weights[index], scales[index], gain, turned_ref)
        for target, dl, place in ((mine_ref, 0, 0), (other_ref, 1, lanes)):
            start = pl.multiple_of((zl ^ dl) * channels, channels)
            place = place + index * channels
            target[place : place + channels, :] = turned_ref[pl.ds(start, channels), :]
    scale = own_row(out_scale_ref[...], rep)
    for index in range(2):
        place = slice(index * lanes, (index + 1) * lanes)
        turned = (out_ref[place, :] * scale).T * own_row(conv_gain_ref[...], index)
        rows = turned.astype(jnp.bfloat16)
        mine_ref[3 * channels :, place] = rows
        other_ref[:lanes, place] = rows


def pair_kernel(spot_ref, *refs):
    weights, scales, gain_ref, targets, turned_ref = refs[:2], refs[2:4], refs[4], refs[5:9], refs[9]
    gain = own_gain(spot_ref, gain_ref)
    for index in range(2):
        turn(spot_ref, weights[index], scales[index], gain, turned_ref)
        units = targets[0].shape[0]
        for dl in range(2):
            start = pl.multiple_of((spot_ref[2] ^ dl) * units, 16)
            targets[2 * index + dl][...] = turned_ref[pl.ds(start, units), :]


def last_kernel(spot_ref, weight_ref, scale_ref, *targets):
    units, width = targets[0].shape
    for chunk in range(2):
        scale = own_row(scale_ref[...], chunk)
        for dl in range(2):
            start = pl.multiple_of((spot_ref[2] ^ dl) * units, 16)
            rows = weight_ref[pl.ds(start, units), chunk * width : (chunk + 1) * width]
            targets[2 * chunk + dl][...] = (rows * scale).astype(jnp.bfloat16)


def mix_kernel(spot_ref, *refs):
    rows, own_ref, twin_ref = refs[:8], refs[8], refs[9]
    taps_ref, mixed_ref, whole_ref, full_ref = refs[10:]
    half, tokens = rows[0].shape
    channels = mixed_ref.shape[0]
    for index in range(4):
        lay_out(spot_ref, index, own_ref[index], full_ref)
        lay_out(spot_ref, index + 4, twin_ref[index], full_ref)
    position = lax.broadcasted_iota(jnp.int32, (channels, tokens), 1) % LEN
    for tile in range(4):
        total = jnp.zeros((3 * channels, tokens), jnp.float32)
        squares = jnp.zeros((1, tokens), jnp.float32)
        spot = pl.multiple_of(tile_of(spot_ref, tile) * tokens, tokens)
        for dx in range(2):
            block = rows[dx * 4 + tile][...]
            start = pl.multiple_of((spot_ref[4] ^ dx) * half, half)
            whole_ref[pl.ds(start, half), pl.ds(spot, tokens)] = block
            total = total + jnp.dot(
                full_ref[:, pl.ds(start, half)], block, preferred_element_type=jnp.float32
            )
            floats = block.astype(jnp.float32)
            squares = squares + jnp.sum(floats * floats, axis=0, keepdims=True)
        total = total * lax.rsqrt(squares / (2 * half) + epsilon)
        u = total[:channels] * total[channels : 2 * channels]
        one = jnp.where(position >= 1, pltpu.roll(u, 1, 1), 0.0)
        two = jnp.where(position >= 2, pltpu.roll(u, 2, 1), 0.0)
        conv = taps_ref[:, 2:3] * u + taps_ref[:, 1:2] * one + taps_ref[:, 0:1] * two
        mixed_ref[:, pl.ds(spot, tokens)] = (total[2 * channels :] * conv).astype(jnp.bfloat16)


def after_kernel(spot_ref, *refs):
    mixed, own_ref, other_ref, twin_ref = refs[:2], *refs[2:5]
    whole_ref, after_ref, kept_ref, full_ref, weight_ref = refs[5:]
    channels, tokens = mixed[0].shape[1:]
    width = weight_ref.shape[0] // 16

    @pl.when(pl.program_id(0) == 0)
    def _():
        for piece in range(4):
            for dy in range(2):
                block = feature_block(spot_ref, piece, dy)
                for dr in range(2):
                    start = pl.multiple_of((block * 2 + (spot_ref[0] ^ dr)) * width, width)
                    for dx in range(2):
                        part = (own_ref, other_ref)[dx][dy, piece]
                        if dr:
                            part = twin_ref[dx, dy, piece]
                        place = slice(dx * 2 * width, (dx + 1) * 2 * width)
                        weight_ref[pl.ds(start, width), place] = part

    squares = jnp.zeros((1, tokens), jnp.float32)
    for dr in range(2):
        for index in range(4):
            block = mixed[dr][index]
            spot = channels_of(spot_ref, (index & 1) * 2 + dr)
            spot = ((index >> 1) * 4 + spot) * channels
            full_ref[pl.ds(pl.multiple_of(spot, channels), channels), :] = block
            floats = block.astype(jnp.float32)
            squares = squares + jnp.sum(floats * floats, axis=0, keepdims=True)
    scale = lax.rsqrt(squares / (8 * channels) + epsilon)
    part = jnp.dot(weight_ref[...], full_ref[...], preferred_element_type=jnp.float32)
    total = whole_ref[...].astype(jnp.float32) + part * scale
    after_ref[...] = total.astype(jnp.bfloat16)

    @pl.when(pl.program_id(0) == tile_of(spot_ref, 0))
    def _():
        half = kept_ref.shape[0]
        start = pl.multiple_of(spot_ref[4] * half, half)
        kept_ref[...] = after_ref[pl.ds(start, half), :]


def norm_scale(rows):
    floats = rows.astype(jnp.float32)
    squares = jnp.sum(floats * floats, axis=0, keepdims=True)
    return lax.rsqrt(squares / rows.shape[0] + epsilon)


def gate_kernel(spot_ref, *refs):
    pieces, after_ref, active_ref, gate_ref = refs[:8], *refs[8:]

    @pl.when(pl.program_id(0) == 0)
    def _():
        for index in range(8):
            lay_out(spot_ref, index, pieces[index][...], gate_ref)

    rows = after_ref[...]
    gate = jnp.dot(gate_ref[...], rows, preferred_element_type=jnp.float32) * norm_scale(rows)
    active_ref[...] = (gate / (1.0 + jnp.exp(-gate))).astype(jnp.bfloat16)


def hidden_kernel(spot_ref, *refs):
    pieces, after_ref, active_ref, hidden_ref, up_ref = refs[:8], *refs[8:]

    @pl.when(pl.program_id(0) == 0)
    def _():
        for index in range(8):
            lay_out(spot_ref, index, pieces[index][...], up_ref)

    rows = after_ref[...]
    upper = jnp.dot(up_ref[...], rows, preferred_element_type=jnp.float32) * norm_scale(rows)
    hidden_ref[...] = (active_ref[...].astype(jnp.float32) * upper).astype(jnp.bfloat16)


def down_kernel(spot_ref, *refs):
    pieces, hidden_ref, outs, full_ref = refs[:8], refs[8], refs[9:11], refs[11]
    half, tokens = outs[0].shape[1:]
    for index in range(8):
        lay_out(spot_ref, index, pieces[index][...], full_ref)
    for dr in (1, 0):
        for dl in range(2):
            spot = pl.multiple_of(tile_of(spot_ref, dl * 2 + dr) * tokens, tokens)
            hidden = hidden_ref[:, pl.ds(spot, tokens)]
            for dx in range(2):
                start = pl.multiple_of((spot_ref[4] ^ dx) * half, half)
                part = lax.dot_general(
                    full_ref[:, pl.ds(start, half)],
                    hidden,
                    (((0,), (0,)), ((), ())),
                    preferred_element_type=jnp.float32,
                )
                outs[dr][dx * 2 + dl] = part.astype(jnp.bfloat16)


def shaped(*shape):
    return jax.ShapeDtypeStruct(shape, jnp.bfloat16)


def whole_blocks(count):
    return [pl.BlockSpec(memory_space=pltpu.VMEM)] * count


def exchanged(
    residual,
    mixer_gain,
    value_weight,
    value_scale,
    input_gate_weight,
    input_gate_scale,
    output_gate_weight,
    output_gate_scale,
    conv_taps,
    conv_gain,
    mixer_out_weight,
    mixer_out_scale,
    channel_gain,
    gate_weight,
    gate_scale,
    up_weight,
    up_scale,
    down_weight,
    down_scale,
):
    axes = ("rep", "zh", "zl", "y", "tp")
    spots = jnp.stack([lax.axis_index(axis) for axis in axes]).astype(jnp.int32)
    half, tokens = residual.shape
    depth = gate_weight.shape[0]
    lanes = depth // 2
    features = 2 * half
    channels = value_weight.shape[1] // 4
    units = gate_weight.shape[1] // 4
    scalars = pl.BlockSpec(memory_space=pltpu.SMEM)
    tile = lambda shape: pl.BlockSpec(shape, lambda i: (0,) * (len(shape) - 1) + (i,))
    fixed = lambda shape: pl.BlockSpec(shape, lambda i: (0,) * len(shape))

    def by_lane(array):
        return array.reshape(-1, lanes)

    def prepare(kernel, operands, half_columns, half_rows, outs, scratch):
        def block(operand):
            if any(operand is weight for weight in half_columns):
                shape = (operand.shape[0], operand.shape[1] // 2)
                return pl.BlockSpec(shape, lambda i, spot_ref: (0, spot_ref[0]))
            if any(operand is weight for weight in half_rows):
                shape = (operand.shape[0] // 2, operand.shape[1])
                return pl.BlockSpec(shape, lambda i, spot_ref: (spot_ref[0], 0))
            return pl.BlockSpec(operand.shape, lambda i, spot_ref: (0, 0))

        return pl.pallas_call(
            kernel,
            out_shape=tuple(shaped(*shape) for shape in outs),
            grid_spec=pltpu.PrefetchScalarGridSpec(
                num_scalar_prefetch=1,
                grid=(1,),
                in_specs=[block(operand) for operand in operands],
                out_specs=tuple(pl.BlockSpec(shape, lambda i, spot_ref: (0, 0)) for shape in outs),
                scratch_shapes=scratch,
            ),
        )(spots, *operands)

    def run(kernel, operands, in_specs, outs, out_specs, scratch, grid=(4,)):
        return pl.pallas_call(
            kernel,
            grid=grid,
            out_shape=outs,
            in_specs=[scalars] + in_specs,
            out_specs=out_specs,
            scratch_shapes=scratch,
        )(spots, *operands)

    def over_z(mine, other):
        return [mine, flip(other, "zl"), flip(mine, "zh"), flip(other, "zh", "zl")]

    def over_y(pieces):
        return pieces + [flip(piece, "y") for piece in pieces]

    rows_zl = flip(residual, "zl")
    rows_tp = flip(residual, "tp")
    rows_both = flip(rows_zl, "tp")
    rows = []
    for block in (residual, rows_zl, rows_tp, rows_both):
        rows = rows + [block, flip(block, "rep")]

    small = (value_weight, input_gate_weight, output_gate_weight)
    mine, other = prepare(
        small_kernel,
        small
        + (by_lane(value_scale), by_lane(input_gate_scale), by_lane(output_gate_scale))
        + (by_lane(mixer_gain), mixer_out_weight, by_lane(conv_gain), by_lane(mixer_out_scale)),
        small + (mixer_out_weight,),
        (),
        [(3 * channels + lanes, depth)] * 2,
        [pltpu.VMEM((lanes, depth), jnp.bfloat16)],
    )
    small_pieces = over_z(mine, other)

    pair = (gate_weight, up_weight)
    pairs = prepare(
        pair_kernel,
        pair + (by_lane(gate_scale), by_lane(up_scale), by_lane(channel_gain)),
        pair,
        (),
        [(units, depth)] * 4,
        [pltpu.VMEM((2 * units, depth), jnp.bfloat16)],
    )
    gates = over_y(over_z(pairs[0], pairs[1]))
    ups = over_y(over_z(pairs[2], pairs[3]))
    downs = prepare(
        last_kernel,
        (down_weight, by_lane(down_scale)),
        (),
        (down_weight,),
        [(units, lanes)] * 4,
        [],
    )
    lasts = over_y(over_z(downs[0], downs[1]))
    lasts = lasts + over_y(over_z(downs[2], downs[3]))
    small_pieces, _ = lax.optimization_barrier((small_pieces, downs[0]))

    places = [lanes * (piece & 1) for piece in range(4)]
    projections = jnp.stack(
        [block[place : place + 3 * channels] for block, place in zip(small_pieces, places)]
    )
    other_projections = flip(projections, "y")
    places = [3 * channels * (1 - (piece & 1)) for piece in range(4)]
    own_out = jnp.stack([block[place : place + lanes] for block, place in zip(small_pieces, places)])
    same_out = flip(own_out, "y")
    place = (lax.axis_index("rep") * 2 + lax.axis_index("zl")) * channels
    own_taps = lax.dynamic_slice_in_dim(conv_taps, place, channels, 1).T
    mixed, whole = run(
        mix_kernel,
        rows[:4] + rows[4:] + [projections, other_projections, own_taps],
        whole_blocks(11),
        (shaped(channels, 4 * tokens), shaped(features, 4 * tokens)),
        tuple(whole_blocks(2)),
        [pltpu.VMEM((3 * channels, features), jnp.bfloat16)],
        grid=(),
    )
    same_out, mixed = lax.optimization_barrier((same_out, mixed))
    out_blocks = jnp.stack([own_out, same_out])
    out_other = flip(out_blocks, "tp")
    out_twin = flip(jnp.stack([out_blocks, out_other]), "rep")
    mixes = jnp.stack([mixed, flip(mixed, "zl"), flip(mixed, "tp"), flip(mixed, "zl", "tp")])
    twin_mixes = flip(mixes, "rep")
    after, after_own = run(
        after_kernel,
        [mixes, twin_mixes, out_blocks, out_other, out_twin, whole],
        [tile((4, channels, tokens))] * 2
        + [fixed(block.shape) for block in (out_blocks, out_other, out_twin)]
        + [tile((features, tokens))],
        (shaped(features, 4 * tokens), shaped(half, tokens)),
        (tile((features, tokens)), fixed((half, tokens))),
        [
            pltpu.VMEM((8 * channels, tokens), jnp.bfloat16),
            pltpu.VMEM((features, 8 * channels), jnp.bfloat16),
        ],
    )

    blocks = [fixed((units, depth))] * 8 + [tile((features, tokens))]
    scratch = [pltpu.VMEM((units, features), jnp.bfloat16)]
    active = run(
        gate_kernel,
        gates + [after],
        blocks,
        shaped(units, 4 * tokens),
        tile((units, tokens)),
        scratch,
    )
    hidden = run(
        hidden_kernel,
        ups + [after, active],
        blocks + [tile((units, tokens))],
        shaped(units, 4 * tokens),
        tile((units, tokens)),
        scratch,
    )
    totals = []
    for chunk in range(2):
        kept, sent = run(
            down_kernel,
            lasts[8 * chunk :][:8] + [hidden],
            whole_blocks(9),
            (shaped(4, half // 2, tokens),) * 2,
            tuple(whole_blocks(2)),
            [pltpu.VMEM((units, half), jnp.bfloat16)],
            grid=(),
        )
        got = flip(sent, "rep")
        own = after_own.reshape(-1, 2, lanes, tokens)[:, chunk].reshape(-1, tokens)
        total = own.astype(jnp.float32) + kept[0].astype(jnp.float32) + got[0].astype(jnp.float32)
        total = lax.optimization_barrier(total)
        for index, way in ((3, ("zl", "tp")), (2, ("tp",)), (1, ("zl",))):
            part = kept[index].astype(jnp.float32) + got[index].astype(jnp.float32)
            part = flip(part.astype(jnp.bfloat16), *way)
            total = total + part.astype(jnp.float32)
        totals.append(total.astype(jnp.bfloat16).reshape(-1, lanes, tokens))
    return jnp.stack(totals, axis=1).reshape(half, tokens)


def solution(mesh):
    sizes = dict(mesh.shape)
    if sizes == {"rep": 2, "fs": 8, "tp": 2}:
        grid = Mesh(mesh.devices.reshape(2, 2, 2, 2, 2), ("rep", "zh", "zl", "y", "tp"))
        fs, step = ("zh", "zl", "y"), exchanged
    else:
        grid, fs, step = mesh, ("fs",), gathered
    own = P("tp", ("rep",) + fs)
    placed = (
        own,
        P(),
        P(fs, "tp"),
        P("tp"),
        P(fs, "tp"),
        P("tp"),
        P(fs, "tp"),
        P("tp"),
        P(None, "tp"),
        P("tp"),
        P("tp", fs),
        P(fs),
        P(),
        P(fs, "tp"),
        P("tp"),
        P(fs, "tp"),
        P("tp"),
        P("tp", fs),
        P(fs),
    )
    step = jax.shard_map(step, mesh=grid, in_specs=placed, out_specs=own, check_vma=False)
    return step
```

```python
import jax
import jax.numpy as jnp
from jax import lax
from jax.experimental import pallas as pl
from jax.experimental.pallas import tpu as pltpu
from jax.sharding import Mesh
from jax.sharding import PartitionSpec as P

LEN = 128


epsilon = 1e-06


def normalize(values, gain):
    floats = values.astype(jnp.float32)
    mean = jnp.mean(floats * floats, axis=0, keepdims=True)
    return (floats * lax.rsqrt(mean + epsilon) * gain[:, None]).astype(jnp.bfloat16)


def contract(weight, rows):
    return lax.dot_general(
        weight, rows, (((0,), (0,)), ((), ())), preferred_element_type=jnp.float32
    )


def causal_conv(values, taps, length):
    total = values.shape[1]
    position = jnp.arange(total, dtype=jnp.int32) % length
    shifted_one = jnp.pad(values, ((0, 0), (1, 0)))[:, :total]
    shifted_two = jnp.pad(values, ((0, 0), (2, 0)))[:, :total]
    shifted_one = jnp.where(position[None, :] >= 1, shifted_one, 0.0)
    shifted_two = jnp.where(position[None, :] >= 2, shifted_two, 0.0)
    return (
        taps[2][:, None] * values + taps[1][:, None] * shifted_one + taps[0][:, None] * shifted_two
    )


def gathered(
    residual,
    mixer_gain,
    value_weight,
    value_scale,
    input_gate_weight,
    input_gate_scale,
    output_gate_weight,
    output_gate_scale,
    conv_taps,
    conv_gain,
    mixer_out_weight,
    mixer_out_scale,
    channel_gain,
    gate_weight,
    gate_scale,
    up_weight,
    up_scale,
    down_weight,
    down_scale,
):
    own_rows = residual.shape[0]
    tokens = residual.shape[1]
    groups = lax.axis_size("tp")
    channels = value_weight.shape[1] * groups
    whole = lax.all_gather(residual, "tp", axis=0, tiled=True)
    normed = normalize(whole, mixer_gain)
    value = contract(
        lax.all_gather(value_weight.astype(jnp.bfloat16), "fs", axis=0, tiled=True), normed
    )
    in_gate = contract(
        lax.all_gather(input_gate_weight.astype(jnp.bfloat16), "fs", axis=0, tiled=True), normed
    )
    out_gate = contract(
        lax.all_gather(output_gate_weight.astype(jnp.bfloat16), "fs", axis=0, tiled=True), normed
    )
    value = value * value_scale[:, None]
    in_gate = in_gate * input_gate_scale[:, None]
    out_gate = out_gate * output_gate_scale[:, None]
    mixed = out_gate * causal_conv(in_gate * value, conv_taps, LEN)
    squares = lax.psum(jnp.sum(mixed * mixed, axis=0), "tp")
    conv_normed = (
        mixed * lax.rsqrt(squares / channels + epsilon)[None, :] * conv_gain[:, None]
    ).astype(jnp.bfloat16)
    out_full = lax.all_gather(mixer_out_weight.astype(jnp.bfloat16), "fs", axis=1, tiled=True)
    out_scale, down_scale_full = (
        lax.all_gather(mixer_out_scale, "fs", axis=0, tiled=True),
        lax.all_gather(down_scale, "fs", axis=0, tiled=True),
    )
    conv_all = lax.all_gather(conv_normed, "tp", axis=0, tiled=True)
    out_own = lax.all_to_all(out_full, "tp", split_axis=1, concat_axis=0, tiled=True)
    block_width = conv_normed.shape[0]
    weight_blocks = out_own.reshape(groups, block_width, own_rows)
    row_blocks = conv_all.reshape(groups, block_width, tokens)
    parts = lax.dot_general(
        weight_blocks, row_blocks, (((1,), (1,)), ((0,), (0,))), preferred_element_type=jnp.float32
    )
    own_scale = lax.dynamic_slice_in_dim(out_scale, lax.axis_index("tp") * own_rows, own_rows, 0)
    rounded = (parts * own_scale[None, :, None]).astype(jnp.bfloat16)
    total = jnp.sum(rounded.astype(jnp.float32), axis=0)
    after_own = (residual.astype(jnp.float32) + total).astype(jnp.bfloat16)
    after_whole = lax.all_gather(after_own, "tp", axis=0, tiled=True)
    normed_two = normalize(after_whole, channel_gain)
    gate_full, up_full = (
        lax.all_gather(gate_weight.astype(jnp.bfloat16), "fs", axis=0, tiled=True),
        lax.all_gather(up_weight.astype(jnp.bfloat16), "fs", axis=0, tiled=True),
    )
    gate = contract(gate_full, normed_two)
    upper = contract(up_full, normed_two)
    hidden = (jax.nn.silu(gate * gate_scale[:, None]) * (upper * up_scale[:, None])).astype(
        jnp.bfloat16
    )
    down_full = lax.all_gather(down_weight.astype(jnp.bfloat16), "fs", axis=1, tiled=True)
    total_two = lax.psum_scatter(
        (contract(down_full, hidden) * down_scale_full[:, None]).astype(jnp.bfloat16),
        "tp",
        scatter_dimension=0,
        tiled=True,
    ).astype(jnp.float32)
    return (after_own.astype(jnp.float32) + total_two).astype(jnp.bfloat16)


def flip(array, *axes):
    count = 2 ** len(axes)
    return lax.ppermute(array, axes, [(i, count - 1 - i) for i in range(count)])


def feature_block(spot_ref, piece, dy):
    zh, zl, y = spot_ref[1], spot_ref[2], spot_ref[3]
    return ((zh ^ (piece >> 1)) * 2 + (zl ^ (piece & 1))) * 2 + (y ^ dy)


def lay_out(spot_ref, index, piece, full_ref):
    width = piece.shape[1]
    start = feature_block(spot_ref, index & 3, index >> 2) * width
    full_ref[:, pl.ds(pl.multiple_of(start, width), width)] = piece


def tile_of(spot_ref, index):
    return (spot_ref[2] ^ (index >> 1)) * 2 + (spot_ref[0] ^ (index & 1))


def channels_of(spot_ref, index):
    return (spot_ref[0] ^ (index & 1)) * 2 + (spot_ref[2] ^ (index >> 1))


def own_row(array, row):
    rows = lax.broadcasted_iota(jnp.int32, array.shape, 0)
    return jnp.sum(jnp.where(rows == row, array, 0.0), axis=0, keepdims=True)


def turn(spot_ref, weight_ref, scale_ref, gain, turned_ref):
    lanes = scale_ref.shape[1]
    scales = scale_ref[...]
    count = weight_ref.shape[1] // lanes
    for index in range(count):
        place = slice(index * lanes, (index + 1) * lanes)
        scaled = weight_ref[:, place] * own_row(scales, spot_ref[0] * count + index)
        turned_ref[place, :] = (scaled.T * gain).astype(jnp.bfloat16)


def own_gain(spot_ref, gain_ref):
    block, gains = feature_block(spot_ref, 0, 0), gain_ref[...]
    return jnp.concatenate([own_row(gains, 2 * block), own_row(gains, 2 * block + 1)], axis=1)


def small_kernel(spot_ref, *refs):
    weights, scales, gain_ref = refs[:3], refs[3:6], refs[6]
    out_ref, conv_gain_ref, out_scale_ref, mine_ref, other_ref, turned_ref = refs[7:]
    rep, zl = spot_ref[0], spot_ref[2]
    lanes = weights[0].shape[1]
    channels = lanes // 2
    gain = own_gain(spot_ref, gain_ref)
    for index in range(3):
        turn(spot_ref, weights[index], scales[index], gain, turned_ref)
        for target, dl, place in ((mine_ref, 0, 0), (other_ref, 1, lanes)):
            start = pl.multiple_of((zl ^ dl) * channels, channels)
            place = place + index * channels
            target[place : place + channels, :] = turned_ref[pl.ds(start, channels), :]
    scale = own_row(out_scale_ref[...], rep)
    for index in range(2):
        place = slice(index * lanes, (index + 1) * lanes)
        turned = (out_ref[place, :] * scale).T * own_row(conv_gain_ref[...], index)
        rows = turned.astype(jnp.bfloat16)
        mine_ref[3 * channels :, place] = rows
        other_ref[:lanes, place] = rows


def pair_kernel(spot_ref, *refs):
    weights, scales, gain_ref, targets, turned_ref = refs[:2], refs[2:4], refs[4], refs[5:9], refs[9]
    gain = own_gain(spot_ref, gain_ref)
    for index in range(2):
        turn(spot_ref, weights[index], scales[index], gain, turned_ref)
        units = targets[0].shape[0]
        for dl in range(2):
            start = pl.multiple_of((spot_ref[2] ^ dl) * units, 16)
            targets[2 * index + dl][...] = turned_ref[pl.ds(start, units), :]


def last_kernel(spot_ref, weight_ref, scale_ref, *targets):
    units, width = targets[0].shape
    for chunk in range(2):
        scale = own_row(scale_ref[...], chunk)
        for dl in range(2):
            start = pl.multiple_of((spot_ref[2] ^ dl) * units, 16)
            rows = weight_ref[pl.ds(start, units), chunk * width : (chunk + 1) * width]
            targets[2 * chunk + dl][...] = (rows * scale).astype(jnp.bfloat16)


def mix_kernel(spot_ref, *refs):
    rows, own_ref, twin_ref = refs[:8], refs[8], refs[9]
    taps_ref, mixed_ref, whole_ref, full_ref = refs[10:]
    half, tokens = rows[0].shape
    channels = mixed_ref.shape[0]
    for index in range(4):
        lay_out(spot_ref, index, own_ref[index], full_ref)
        lay_out(spot_ref, index + 4, twin_ref[index], full_ref)
    position = lax.broadcasted_iota(jnp.int32, (channels, tokens), 1) % LEN
    for tile in range(4):
        total = jnp.zeros((3 * channels, tokens), jnp.float32)
        squares = jnp.zeros((1, tokens), jnp.float32)
        spot = pl.multiple_of(tile_of(spot_ref, tile) * tokens, tokens)
        for dx in range(2):
            block = rows[dx * 4 + tile][...]
            start = pl.multiple_of((spot_ref[4] ^ dx) * half, half)
            whole_ref[pl.ds(start, half), pl.ds(spot, tokens)] = block
            total = total + jnp.dot(
                full_ref[:, pl.ds(start, half)], block, preferred_element_type=jnp.float32
            )
            floats = block.astype(jnp.float32)
            squares = squares + jnp.sum(floats * floats, axis=0, keepdims=True)
        total = total * lax.rsqrt(squares / (2 * half) + epsilon)
        u = total[:channels] * total[channels : 2 * channels]
        one = jnp.where(position >= 1, pltpu.roll(u, 1, 1), 0.0)
        two = jnp.where(position >= 2, pltpu.roll(u, 2, 1), 0.0)
        conv = taps_ref[:, 2:3] * u + taps_ref[:, 1:2] * one + taps_ref[:, 0:1] * two
        mixed_ref[:, pl.ds(spot, tokens)] = (total[2 * channels :] * conv).astype(jnp.bfloat16)


def after_kernel(spot_ref, *refs):
    mixed, own_ref, other_ref, twin_ref = refs[:2], *refs[2:5]
    whole_ref, after_ref, kept_ref, full_ref, weight_ref = refs[5:]
    channels, tokens = mixed[0].shape[1:]
    width = weight_ref.shape[0] // 16

    @pl.when(pl.program_id(0) == 0)
    def _():
        for piece in range(4):
            for dy in range(2):
                block = feature_block(spot_ref, piece, dy)
                for dr in range(2):
                    start = pl.multiple_of((block * 2 + (spot_ref[0] ^ dr)) * width, width)
                    for dx in range(2):
                        part = (own_ref, other_ref)[dx][dy, piece]
                        if dr:
                            part = twin_ref[dx, dy, piece]
                        place = slice(dx * 2 * width, (dx + 1) * 2 * width)
                        weight_ref[pl.ds(start, width), place] = part

    squares = jnp.zeros((1, tokens), jnp.float32)
    for dr in range(2):
        for index in range(4):
            block = mixed[dr][index]
            spot = channels_of(spot_ref, (index & 1) * 2 + dr)
            spot = ((index >> 1) * 4 + spot) * channels
            full_ref[pl.ds(pl.multiple_of(spot, channels), channels), :] = block
            floats = block.astype(jnp.float32)
            squares = squares + jnp.sum(floats * floats, axis=0, keepdims=True)
    scale = lax.rsqrt(squares / (8 * channels) + epsilon)
    part = jnp.dot(weight_ref[...], full_ref[...], preferred_element_type=jnp.float32)
    total = whole_ref[...].astype(jnp.float32) + part * scale
    after_ref[...] = total.astype(jnp.bfloat16)

    @pl.when(pl.program_id(0) == tile_of(spot_ref, 0))
    def _():
        half = kept_ref.shape[0]
        start = pl.multiple_of(spot_ref[4] * half, half)
        kept_ref[...] = after_ref[pl.ds(start, half), :]


def norm_scale(rows):
    floats = rows.astype(jnp.float32)
    squares = jnp.sum(floats * floats, axis=0, keepdims=True)
    return lax.rsqrt(squares / rows.shape[0] + epsilon)


def gate_kernel(spot_ref, *refs):
    pieces, after_ref, active_ref, gate_ref = refs[:8], *refs[8:]

    @pl.when(pl.program_id(0) == 0)
    def _():
        for index in range(8):
            lay_out(spot_ref, index, pieces[index][...], gate_ref)

    rows = after_ref[...]
    gate = jnp.dot(gate_ref[...], rows, preferred_element_type=jnp.float32) * norm_scale(rows)
    active_ref[...] = (gate / (1.0 + jnp.exp(-gate))).astype(jnp.bfloat16)


def hidden_kernel(spot_ref, *refs):
    pieces, after_ref, active_ref, hidden_ref, up_ref = refs[:8], *refs[8:]

    @pl.when(pl.program_id(0) == 0)
    def _():
        for index in range(8):
            lay_out(spot_ref, index, pieces[index][...], up_ref)

    rows = after_ref[...]
    upper = jnp.dot(up_ref[...], rows, preferred_element_type=jnp.float32) * norm_scale(rows)
    hidden_ref[...] = (active_ref[...].astype(jnp.float32) * upper).astype(jnp.bfloat16)


def down_kernel(spot_ref, *refs):
    pieces, hidden_ref, outs, full_ref = refs[:8], refs[8], refs[9:11], refs[11]
    half, tokens = outs[0].shape[1:]
    for index in range(8):
        lay_out(spot_ref, index, pieces[index][...], full_ref)
    for dr in (1, 0):
        for dl in range(2):
            spot = pl.multiple_of(tile_of(spot_ref, dl * 2 + dr) * tokens, tokens)
            hidden = hidden_ref[:, pl.ds(spot, tokens)]
            for dx in range(2):
                start = pl.multiple_of((spot_ref[4] ^ dx) * half, half)
                part = lax.dot_general(
                    full_ref[:, pl.ds(start, half)],
                    hidden,
                    (((0,), (0,)), ((), ())),
                    preferred_element_type=jnp.float32,
                )
                outs[dr][dx * 2 + dl] = part.astype(jnp.bfloat16)


def shaped(*shape):
    return jax.ShapeDtypeStruct(shape, jnp.bfloat16)


def whole_blocks(count):
    return [pl.BlockSpec(memory_space=pltpu.VMEM)] * count


def exchanged(
    residual,
    mixer_gain,
    value_weight,
    value_scale,
    input_gate_weight,
    input_gate_scale,
    output_gate_weight,
    output_gate_scale,
    conv_taps,
    conv_gain,
    mixer_out_weight,
    mixer_out_scale,
    channel_gain,
    gate_weight,
    gate_scale,
    up_weight,
    up_scale,
    down_weight,
    down_scale,
):
    axes = ("rep", "zh", "zl", "y", "tp")
    spots = jnp.stack([lax.axis_index(axis) for axis in axes]).astype(jnp.int32)
    half, tokens = residual.shape
    depth = gate_weight.shape[0]
    lanes = depth // 2
    features = 2 * half
    channels = value_weight.shape[1] // 4
    units = gate_weight.shape[1] // 4
    scalars = pl.BlockSpec(memory_space=pltpu.SMEM)
    tile = lambda shape: pl.BlockSpec(shape, lambda i: (0,) * (len(shape) - 1) + (i,))
    fixed = lambda shape: pl.BlockSpec(shape, lambda i: (0,) * len(shape))

    def by_lane(array):
        return array.reshape(-1, lanes)

    def prepare(kernel, operands, half_columns, half_rows, outs, scratch):
        def block(operand):
            if any(operand is weight for weight in half_columns):
                shape = (operand.shape[0], operand.shape[1] // 2)
                return pl.BlockSpec(shape, lambda i, spot_ref: (0, spot_ref[0]))
            if any(operand is weight for weight in half_rows):
                shape = (operand.shape[0] // 2, operand.shape[1])
                return pl.BlockSpec(shape, lambda i, spot_ref: (spot_ref[0], 0))
            return pl.BlockSpec(operand.shape, lambda i, spot_ref: (0, 0))

        return pl.pallas_call(
            kernel,
            out_shape=tuple(shaped(*shape) for shape in outs),
            grid_spec=pltpu.PrefetchScalarGridSpec(
                num_scalar_prefetch=1,
                grid=(1,),
                in_specs=[block(operand) for operand in operands],
                out_specs=tuple(pl.BlockSpec(shape, lambda i, spot_ref: (0, 0)) for shape in outs),
                scratch_shapes=scratch,
            ),
        )(spots, *operands)

    def run(kernel, operands, in_specs, outs, out_specs, scratch, grid=(4,)):
        return pl.pallas_call(
            kernel,
            grid=grid,
            out_shape=outs,
            in_specs=[scalars] + in_specs,
            out_specs=out_specs,
            scratch_shapes=scratch,
        )(spots, *operands)

    def over_z(mine, other):
        return [mine, flip(other, "zl"), flip(mine, "zh"), flip(other, "zh", "zl")]

    def over_y(pieces):
        return pieces + [flip(piece, "y") for piece in pieces]

    rows_zl = flip(residual, "zl")
    rows_tp = flip(residual, "tp")
    rows_both = flip(rows_zl, "tp")
    rows = []
    for block in (residual, rows_zl, rows_tp, rows_both):
        rows = rows + [block, flip(block, "rep")]

    small = (value_weight, input_gate_weight, output_gate_weight)
    mine, other = prepare(
        small_kernel,
        small
        + (by_lane(value_scale), by_lane(input_gate_scale), by_lane(output_gate_scale))
        + (by_lane(mixer_gain), mixer_out_weight, by_lane(conv_gain), by_lane(mixer_out_scale)),
        small + (mixer_out_weight,),
        (),
        [(3 * channels + lanes, depth)] * 2,
        [pltpu.VMEM((lanes, depth), jnp.bfloat16)],
    )
    small_pieces = over_z(mine, other)

    pair = (gate_weight, up_weight)
    pairs = prepare(
        pair_kernel,
        pair + (by_lane(gate_scale), by_lane(up_scale), by_lane(channel_gain)),
        pair,
        (),
        [(units, depth)] * 4,
        [pltpu.VMEM((2 * units, depth), jnp.bfloat16)],
    )
    gates = over_y(over_z(pairs[0], pairs[1]))
    ups = over_y(over_z(pairs[2], pairs[3]))
    downs = prepare(
        last_kernel,
        (down_weight, by_lane(down_scale)),
        (),
        (down_weight,),
        [(units, lanes)] * 4,
        [],
    )
    lasts = over_y(over_z(downs[0], downs[1]))
    lasts = lasts + over_y(over_z(downs[2], downs[3]))
    small_pieces, _ = lax.optimization_barrier((small_pieces, downs[0]))

    places = [lanes * (piece & 1) for piece in range(4)]
    projections = jnp.stack(
        [block[place : place + 3 * channels] for block, place in zip(small_pieces, places)]
    )
    other_projections = flip(projections, "y")
    places = [3 * channels * (1 - (piece & 1)) for piece in range(4)]
    own_out = jnp.stack([block[place : place + lanes] for block, place in zip(small_pieces, places)])
    same_out = flip(own_out, "y")
    place = (lax.axis_index("rep") * 2 + lax.axis_index("zl")) * channels
    own_taps = lax.dynamic_slice_in_dim(conv_taps, place, channels, 1).T
    mixed, whole = run(
        mix_kernel,
        rows[:4] + rows[4:] + [projections, other_projections, own_taps],
        whole_blocks(11),
        (shaped(channels, 4 * tokens), shaped(features, 4 * tokens)),
        tuple(whole_blocks(2)),
        [pltpu.VMEM((3 * channels, features), jnp.bfloat16)],
        grid=(),
    )
    same_out, mixed = lax.optimization_barrier((same_out, mixed))
    out_blocks = jnp.stack([own_out, same_out])
    out_other = flip(out_blocks, "tp")
    out_twin = flip(jnp.stack([out_blocks, out_other]), "rep")
    mixes = jnp.stack([mixed, flip(mixed, "zl"), flip(mixed, "tp"), flip(mixed, "zl", "tp")])
    twin_mixes = flip(mixes, "rep")
    after, after_own = run(
        after_kernel,
        [mixes, twin_mixes, out_blocks, out_other, out_twin, whole],
        [tile((4, channels, tokens))] * 2
        + [fixed(block.shape) for block in (out_blocks, out_other, out_twin)]
        + [tile((features, tokens))],
        (shaped(features, 4 * tokens), shaped(half, tokens)),
        (tile((features, tokens)), fixed((half, tokens))),
        [
            pltpu.VMEM((8 * channels, tokens), jnp.bfloat16),
            pltpu.VMEM((features, 8 * channels), jnp.bfloat16),
        ],
    )

    blocks = [fixed((units, depth))] * 8 + [tile((features, tokens))]
    scratch = [pltpu.VMEM((units, features), jnp.bfloat16)]
    active = run(
        gate_kernel,
        gates + [after],
        blocks,
        shaped(units, 4 * tokens),
        tile((units, tokens)),
        scratch,
    )
    hidden = run(
        hidden_kernel,
        ups + [after, active],
        blocks + [tile((units, tokens))],
        shaped(units, 4 * tokens),
        tile((units, tokens)),
        scratch,
    )
    out = jnp.zeros((half // depth, 2, lanes, tokens), jnp.bfloat16)
    for chunk in range(2):
        kept, sent = run(
            down_kernel,
            lasts[8 * chunk :][:8] + [hidden],
            whole_blocks(9),
            (shaped(4, half // 2, tokens),) * 2,
            tuple(whole_blocks(2)),
            [pltpu.VMEM((units, half), jnp.bfloat16)],
            grid=(),
        )
        got = flip(sent, "rep")
        own = after_own.reshape(-1, 2, lanes, tokens)[:, chunk].reshape(-1, tokens)
        total = own.astype(jnp.float32) + kept[0].astype(jnp.float32) + got[0].astype(jnp.float32)
        total = lax.optimization_barrier(total)
        for index, way in ((3, ("zl", "tp")), (2, ("tp",)), (1, ("zl",))):
            part = kept[index].astype(jnp.float32) + got[index].astype(jnp.float32)
            part = flip(part.astype(jnp.bfloat16), *way)
            total = total + part.astype(jnp.float32)
        total = total.astype(jnp.bfloat16).reshape(-1, 1, lanes, tokens)
        out = lax.dynamic_update_slice_in_dim(out, total, chunk, 1)
    return out.reshape(half, tokens)


def solution(mesh):
    sizes = dict(mesh.shape)
    if sizes == {"rep": 2, "fs": 8, "tp": 2}:
        grid = Mesh(mesh.devices.reshape(2, 2, 2, 2, 2), ("rep", "zh", "zl", "y", "tp"))
        fs, step = ("zh", "zl", "y"), exchanged
    else:
        grid, fs, step = mesh, ("fs",), gathered
    own = P("tp", ("rep",) + fs)
    placed = (
        own,
        P(),
        P(fs, "tp"),
        P("tp"),
        P(fs, "tp"),
        P("tp"),
        P(fs, "tp"),
        P("tp"),
        P(None, "tp"),
        P("tp"),
        P("tp", fs),
        P(fs),
        P(),
        P(fs, "tp"),
        P("tp"),
        P(fs, "tp"),
        P("tp"),
        P("tp", fs),
        P(fs),
    )
    step = jax.shard_map(step, mesh=grid, in_specs=placed, out_specs=own, check_vma=False)
    return step
```
